512 devices in a mesh: ep: 128 (over z, y, core), tp: 4 (over x).
Axes of the slice: x: 4, y: 8, z: 8, core: 2. Of those that a mesh axis runs over, the one named last changes fastest.
Arguments:
- residual_in: bfloat16 [2560, 1024], P('ep', 'tp'), may hold values from -64 to 64
- queries: bfloat16 [2560, 512], P(('ep', 'tp')), may hold values from -6 to 6
- cache_keys: bfloat16 [2560, 1024, 128], P(('ep', 'tp')), may hold values from -6 to 6
- cache_values: bfloat16 [2560, 1024, 128], P(('ep', 'tp')), may hold values from -24 to 24
- lengths: int32 [2560], P(('ep', 'tp')), may hold values from 256 to 1024
- stick_offset: float32 [8], replicated, may hold values from 0.5 to 6
- out_weight: bfloat16 [512, 1024], P(None, 'tp'), may hold values from -0.25 to 0.25
- norm1_gain: float32 [1024], P('tp'), may hold values from 0.3 to 3.1
- norm1_bias: float32 [1024], P('tp'), may hold values from -1.5 to 1.5
- routes: int32 [2560, 6], P('ep'), may hold values from 0 to 127, all different within a row; in each aligned block of 20 rows (0 to 19, 20 to 39, ...) at most 2 rows name the same one
- route_weights: float32 [2560, 6], P('ep'), may hold values from 0.1 to 0.8
- expert_gate: bfloat16 [128, 1024, 512], P('ep', None, 'tp'), may hold values from -0.1875 to 0.1875
- expert_up: bfloat16 [128, 1024, 512], P('ep', None, 'tp'), may hold values from -0.1875 to 0.1875
- expert_down: bfloat16 [128, 512, 1024], P('ep', 'tp'), may hold values from -0.25 to 0.25
- shared_gate: bfloat16 [1024, 512], P(None, 'tp'), may hold values from -0.1875 to 0.1875
- shared_up: bfloat16 [1024, 512], P(None, 'tp'), may hold values from -0.1875 to 0.1875
- shared_down: bfloat16 [512, 1024], P('tp'), may hold values from -0.25 to 0.25
- norm2_gain: float32 [1024], P('tp'), may hold values from 0.1 to 1.9
- norm2_bias: float32 [1024], P('tp'), may hold values from -1.5 to 1.5
Outputs:
- layer_out: bfloat16 [2560, 1024], P('ep', 'tp')
The draws below stay inside these ranges and needn't reach their ends.
Inputs may be any that keep to these rules, and one draw needn't show every extreme that they name: `routes`: each row names 6 different experts; among the rows of one index of ep no expert is named more than 2 times.
All inputs are finite; a program needn't handle non-finite values.
Results may differ from the reference program's by a relative error of at most 0.0095.
Values may be sent and summed in bfloat16 or wider, within the bound.
No kernel may reach another device: no remote copies, remote signals or barrier semaphores. Data moves between devices by JAX's collectives and lax.ppermute only.
A program may use at most 64 MiB of HBM per device.

```python
import math
import jax
import jax.numpy as jnp
import numpy as np
from jax import lax

D = 1024
H = 8
HD = 64
KVH = 2
CACHE = 1024
FE = 512
FS = 512
TOPK = 6
SEQ_DEV = 20
SEQS = 2560
EXPERTS = 128
CAP = 2
FE_DEV = 128
N_EP = 128
N_TP = 4


def draw_residual_in(key, part):
    key_entries, key_scale = jax.random.split(key, 2)
    places = jnp.arange(D, dtype=jnp.float32) / D
    column_scale = jnp.exp(1.4 * places) * jax.random.uniform(key_scale, (D,), jnp.float32, 0.6, 1.5)
    entries = jnp.clip(jax.random.normal(key_entries, (SEQS, D), jnp.float32), -5.0, 5.0)
    return (entries * column_scale).astype(jnp.bfloat16)


def draw_norm1_gain(key, part):
    places = jnp.arange(D, dtype=jnp.float32) / D
    roughness = jax.random.uniform(key, (D,), jnp.float32, 0.8, 1.25)
    rising = 0.5 * jnp.exp(1.4 * places)
    return rising * roughness


def touch_ends(values, stream_key, low, high):
    spot = [jax.random.randint(jax.random.fold_in(stream_key, axis), (), 0, length) for axis, length in enumerate(values.shape)]
    main_axis = values.shape.index(max(values.shape))
    neighbour = spot[:main_axis] + [(spot[main_axis] + 1) % values.shape[main_axis]] + spot[main_axis + 1:]
    return values.at[tuple(spot)].set(low).at[tuple(neighbour)].set(high)


def levels(rng, extent, shards, smallest, top_value):
    level = 1.0
    for dim, blocks in shards:
        draws = jax.random.uniform(jax.random.fold_in(jax.random.fold_in(rng, 6), dim), (blocks,), jnp.float32, smallest / len(shards), top_value / len(shards))
        level = level * jnp.repeat(jnp.exp(draws), extent[dim] // blocks).reshape((-1,) + (1,) * (len(extent) - 1 - dim))
    return level


def routed_block(rng, own, number, rows, number_of, top, most, lean):
    order = jax.random.permutation(rng, number_of)
    heavy_load, usual = portions_of(number_of, rows * top, most, lean, True), portions_of(number_of, rows * top, most, lean, False)
    places = jnp.arange(number_of)

    def named(sizes, rotation):
        used = int((sizes > 0).sum())
        fixed = max(1, used // 4)
        shifted = fixed + (places - fixed + rotation * (used - fixed)) % max(1, number_of - fixed)
        return jnp.zeros((number_of,), jnp.int32).at[order[jnp.where(places < fixed, places, shifted)]].set(jnp.asarray(sizes, jnp.int32))

    sizes = jnp.where(number % 4 == 0, named(heavy_load, number // 4), named(usual, number - number // 4 - 1))
    mixed = jax.random.permutation(jax.random.fold_in(own, 3), number_of)
    donor, receiver = mixed[0:number_of // 2 * 2:2], mixed[1:number_of // 2 * 2:2]
    slack = jnp.minimum(sizes[donor] - 1, most - sizes[receiver]) // 2
    slack = jnp.where((donor == order[0]) | (receiver == order[0]) | (sizes[receiver] == 0), 0, jnp.maximum(slack, 0))
    shifted = jax.random.randint(jax.random.fold_in(own, 4), (number_of // 2,), 0, 1 << 20) % (slack + 1)
    sizes = sizes.at[donor].add(-shifted).at[receiver].add(shifted)
    items = jnp.searchsorted(jnp.cumsum(sizes), jnp.arange(rows * top), side="right").astype(jnp.int32)
    listing = items.reshape(top, rows).T
    listing = listing[jax.random.permutation(jax.random.fold_in(own, 1), rows)]
    rotation = jax.random.randint(jax.random.fold_in(own, 2), (rows, 1), 0, top)
    return jnp.take_along_axis(listing, (jnp.arange(top)[None, :] + rotation) % top, axis=1)


def portions_of(number_of, total, most, slope, full):
    loads = [(1 << 20) // math.isqrt(rank ** slope) + 1 for rank in range(1, number_of + 1)]
    largest = most if full else min(most, max(-(-total // number_of), total * loads[0] // sum(loads)))
    least = 1 if total - largest >= number_of - 1 else 0
    counts, rest = [largest] + [least] * (number_of - 1), total - largest - least * (number_of - 1)
    while rest > 0:
        movable = [i for i in range(1, number_of) if counts[i] < largest] or [i for i in range(1, number_of) if counts[i] < most]
        pool, budget = sum([loads[i] for i in movable]), rest
        for i in movable:
            addition = min(most - counts[i], max(1, budget * loads[i] // pool), rest)
            counts[i] = counts[i] + addition
            rest = rest - addition
    return np.array(counts)


def noise(rng, extent, deviation, reach, cuts=(), kind=jnp.bfloat16):
    level = levels(rng, extent, cuts, -0.22, 0.18) if cuts else 1.0
    drawn = jax.random.normal(rng, extent, jnp.float32) * deviation * level
    return jnp.minimum(jnp.maximum(drawn, -reach), reach).astype(kind)


def setup_inputs(seed: int = 0) -> dict:
    key_list = jax.random.split(jax.random.key(seed), 20)
    residual_in = draw_residual_in(jax.random.fold_in(key_list[19], 71), 0)
    queries = noise(key_list[1], (SEQS, H * HD), 1.0, 6.0, ((0, 512),))
    cache_keys = noise(key_list[2], (SEQS, CACHE, KVH * HD), 1.0, 6.0, ((0, 512),))
    cache_values = noise(key_list[3], (SEQS, CACHE, KVH * HD), 4.0, 24.0, ((0, 512),))
    lengths = touch_ends(jax.random.randint(key_list[4], (SEQS,), CACHE // 4, CACHE + 1), jax.random.fold_in(key_list[4], 1), CACHE // 4, CACHE).astype(jnp.int32)
    stick_offset = jnp.clip(jnp.exp(jax.random.uniform(key_list[5], (H,), jnp.float32, math.log(0.5), math.log(6.0))), 0.5, 6.0)
    out_weight = noise(key_list[6], (H * HD, D), (H * HD) ** -0.5, 0.25, ((1, 4),))
    norm1_gain = draw_norm1_gain(jax.random.fold_in(key_list[19], 71), 0)
    norm1_bias = noise(key_list[8], (D,), 0.3, 1.5, ((0, 4),), jnp.float32)
    routes_keys = jax.random.split(jax.random.fold_in(key_list[9], 1), SEQS // SEQ_DEV)
    routes_turns = jax.random.permutation(jax.random.fold_in(key_list[9], 3), SEQS // SEQ_DEV)
    routes = jax.vmap(lambda own, number: routed_block(jax.random.fold_in(key_list[9], 2), own, number, SEQ_DEV, EXPERTS, TOPK, CAP, 2))(routes_keys, routes_turns).reshape((SEQS, TOPK))
    route_weights = jnp.clip(0.1 + 0.7 * jax.random.uniform(key_list[10], (SEQS, TOPK), jnp.float32) ** levels(key_list[10], (SEQS, TOPK), ((0, 128),), -0.2, 0.2), 0.1, 0.8)
    expert_gate = noise(key_list[11], (EXPERTS, D, FE), D ** -0.5, 0.1875, ((0, 128), (2, 4)))
    expert_up = noise(key_list[12], (EXPERTS, D, FE), D ** -0.5, 0.1875, ((0, 128), (2, 4)))
    expert_down = noise(key_list[13], (EXPERTS, FE, D), FE ** -0.5, 0.25, ((0, 128), (1, 4)))
    shared_gate = noise(key_list[14], (D, FS), D ** -0.5, 0.1875, ((1, 4),))
    shared_up = noise(key_list[15], (D, FS), D ** -0.5, 0.1875, ((1, 4),))
    shared_down = noise(key_list[16], (FS, D), FS ** -0.5, 0.25, ((0, 4),))
    norm2_gain = jnp.clip(1.0 + 0.18 * jax.random.normal(key_list[17], (D,), jnp.float32), 0.1, 1.9)
    norm2_bias = noise(key_list[18], (D,), 0.3, 1.5, ((0, 4),), jnp.float32)
    return dict(residual_in=residual_in, queries=queries, cache_keys=cache_keys, cache_values=cache_values, lengths=lengths, stick_offset=stick_offset, out_weight=out_weight, norm1_gain=norm1_gain, norm1_bias=norm1_bias, routes=routes, route_weights=route_weights, expert_gate=expert_gate, expert_up=expert_up, expert_down=expert_down, shared_gate=shared_gate, shared_up=shared_up, shared_down=shared_down, norm2_gain=norm2_gain, norm2_bias=norm2_bias)


RESIDUAL_SCALE = 2.0 ** 0.25
EPSILON = 1e-05

def normalize(totals, squares, entries, values, scales, shifts):
    centre = totals / entries
    spread = squares / entries - centre * centre
    return (values - centre) * lax.rsqrt(spread + EPSILON) * scales + shifts

def stick_read(queries, keys_block, values_block, lengths, offsets):
    seq_count = queries.shape[0]
    grouped = H // KVH
    query_heads = queries.astype(jnp.float32).reshape(seq_count, KVH, grouped, HD)
    key_heads = keys_block.astype(jnp.float32).reshape(seq_count, CACHE, KVH, HD)
    value_heads = values_block.astype(jnp.float32).reshape(seq_count, CACHE, KVH, HD)
    scores = jnp.einsum('sgjd,slgd->sgjl', query_heads, key_heads) * HD ** (-0.5)
    scores = scores - offsets.reshape(1, KVH, grouped, 1)
    live_mask = (jnp.arange(CACHE)[None, :] < lengths[:, None])[:, None, None, :]
    keep_log = jnp.where(live_mask, jax.nn.log_sigmoid(-scores), 0.0)
    after_log = lax.cumsum(keep_log, axis=3, reverse=True) - keep_log
    weights = jnp.where(live_mask, jnp.exp(jax.nn.log_sigmoid(scores) + after_log), 0.0)
    weights = lax.optimization_barrier(weights.astype(jnp.bfloat16)).astype(jnp.float32)
    mixed = jnp.einsum('sgjl,slgd->sgjd', weights, value_heads)
    return mixed.reshape(seq_count, H * HD).astype(jnp.bfloat16)

def reference(residual_in, queries, cache_keys, cache_values, lengths, stick_offset, out_weight, norm1_gain, norm1_bias, routes, route_weights, expert_gate, expert_up, expert_down, shared_gate, shared_up, shared_down, norm2_gain, norm2_bias):
    blocks = N_EP * N_TP
    per_block = SEQ_DEV // N_TP

    def read_block(members):
        return stick_read(members[0], members[1], members[2], members[3], stick_offset)
    mixed = lax.map(read_block, (queries.reshape(blocks, per_block, H * HD), cache_keys.reshape(blocks, per_block, CACHE, KVH * HD), cache_values.reshape(blocks, per_block, CACHE, KVH * HD), lengths.reshape(blocks, per_block)))
    mixed = mixed.reshape(SEQS, H * HD)
    before = RESIDUAL_SCALE * residual_in.astype(jnp.float32) + jnp.dot(mixed, out_weight, preferred_element_type=jnp.float32)
    normed = normalize(lax.optimization_barrier(jnp.sum(before, axis=1, keepdims=True)), lax.optimization_barrier(jnp.sum(before * before, axis=1, keepdims=True)), D, before, norm1_gain, norm1_bias).astype(jnp.bfloat16)
    normed = lax.optimization_barrier(normed)
    assign = SEQ_DEV * TOPK
    slots_all = EXPERTS * CAP
    chosen = routes.reshape(N_EP, assign)
    order_ids = jnp.arange(assign)
    earlier = order_ids[None, :] < order_ids[:, None]

    def slot_of(flat):
        matches = (flat[:, None] == flat[None, :]) & earlier
        return lax.optimization_barrier(jnp.sum(matches.astype(jnp.int32), axis=1))
    slot_ids = jax.vmap(slot_of)(chosen)
    targets = chosen * CAP + slot_ids
    picks = (targets[:, :, None] == jnp.arange(slots_all)[None, None, :]).astype(jnp.float32)
    picks = picks.reshape(N_EP, SEQ_DEV, TOPK, slots_all)
    dispatch = lax.optimization_barrier(jnp.sum(picks, axis=2))
    combine = lax.optimization_barrier(jnp.sum(picks * route_weights.reshape(N_EP, SEQ_DEV, TOPK, 1), axis=2))
    rows_in = jnp.einsum('gsr,gsd->grd', dispatch, normed.reshape(N_EP, SEQ_DEV, D).astype(jnp.float32), precision=lax.Precision.HIGHEST)
    rows_in = rows_in.reshape(N_EP, EXPERTS, CAP, D).transpose(1, 0, 2, 3)
    rows_in = rows_in.reshape(EXPERTS, N_EP * CAP, D).astype(jnp.bfloat16)

    def run_expert(members):
        arrived, gate_weight, up_weight, down_weight = members
        gate_part = jnp.dot(arrived, gate_weight, preferred_element_type=jnp.float32)
        up_part = jnp.dot(arrived, up_weight, preferred_element_type=jnp.float32)
        hidden = lax.optimization_barrier((jax.nn.silu(gate_part) * up_part).astype(jnp.bfloat16))
        blocked = hidden.astype(jnp.float32).reshape(N_EP * CAP, N_TP, FE_DEV)
        partial_value = jnp.einsum('rtf,tfd->trd', blocked, down_weight.astype(jnp.float32).reshape(N_TP, FE_DEV, D))
        partial_value = lax.optimization_barrier(partial_value.astype(jnp.bfloat16)).astype(jnp.float32)
        return lax.optimization_barrier(jnp.sum(partial_value, axis=0)).astype(jnp.bfloat16)
    produced = lax.map(run_expert, (rows_in, expert_gate, expert_up, expert_down))
    produced = produced.reshape(EXPERTS, N_EP, CAP, D).transpose(1, 0, 2, 3)
    produced = produced.reshape(N_EP, slots_all, D).astype(jnp.float32)
    routed = jnp.einsum('gsr,grd->gsd', combine, produced, precision=lax.Precision.HIGHEST).reshape(SEQS, D)
    shared_hidden = (jax.nn.silu(jnp.dot(normed, shared_gate, preferred_element_type=jnp.float32)) * jnp.dot(normed, shared_up, preferred_element_type=jnp.float32)).astype(jnp.bfloat16)
    shared = jnp.dot(shared_hidden, shared_down, preferred_element_type=jnp.float32)
    after = RESIDUAL_SCALE * normed.astype(jnp.float32) + routed + shared
    return normalize(lax.optimization_barrier(jnp.sum(after, axis=1, keepdims=True)), lax.optimization_barrier(jnp.sum(after * after, axis=1, keepdims=True)), D, after, norm2_gain, norm2_bias).astype(jnp.bfloat16)
```

```python
import jax
import jax.numpy as jnp
from jax import lax
from jax.experimental import pallas as pl
from jax.experimental.pallas import tpu as pltpu
from jax.sharding import PartitionSpec as P

H = 8
HD = 64
KVH = 2
CACHE = 1024
TOPK = 6
LANES = 128
BLOCKS = CACHE // LANES

RESIDUAL_SCALE = 2.0**0.25
EPSILON = 1e-05


def stick_kernel(
    lengths, offsets, queries, keys, values, gate, up, down,
    out, packed, keys_vm, values_vm, reads, key_sems, value_sems, pack_sems,
):
    seqs = queries.shape[0]
    wide, hidden = gate.shape[1], gate.shape[2]
    key_copies = [
        pltpu.make_async_copy(keys.at[s], keys_vm.at[s], key_sems.at[s]) for s in range(seqs)
    ]
    value_copies = [
        pltpu.make_async_copy(values.at[s], values_vm.at[s], value_sems.at[s])
        for s in range(seqs)
    ]
    pieces = [(gate.at[0], 0, wide), (up.at[0], wide, wide)]
    for j in range(wide // LANES):
        piece = down.at[0, :, pl.ds(j * LANES, LANES)]
        pieces.append((piece, 2 * wide + j * hidden, hidden))
    pack_copies = [
        pltpu.make_async_copy(piece, packed.at[pl.ds(at, rows)], pack_sems.at[i])
        for i, (piece, at, rows) in enumerate(pieces)
    ]
    for copy in key_copies + value_copies + pack_copies:
        copy.start()

    row = lax.broadcasted_iota(jnp.int32, (H, LANES), 0)
    lane = lax.broadcasted_iota(jnp.int32, (H, LANES), 1)
    low = lane < HD
    first = row < H // KVH
    offset = jnp.zeros((H, LANES), jnp.float32)
    for h in range(H):
        offset = jnp.where(row == h, offsets[h], offset)
    wide_q = queries[...].astype(jnp.float32)
    place = lax.broadcasted_iota(jnp.int32, (LANES, 2 * LANES), 0)
    column = lax.broadcasted_iota(jnp.int32, (LANES, 2 * LANES), 1)
    later = jnp.where((place > column) | (column >= LANES), 1.0, 0.0).astype(jnp.bfloat16)

    stays, takes = [], []
    for s in range(seqs):
        query = jnp.zeros((H, LANES), jnp.float32)
        for h in range(H):
            pair = lax.slice(wide_q, (s, h // 2 * LANES), (s + 1, (h // 2 + 1) * LANES))
            both = jnp.broadcast_to(pair, (H, LANES))
            if h % 2 != h // (H // KVH):
                both = pltpu.roll(both, HD, 1)
            query = jnp.where(row == h, both, query)
        query = jnp.where(first == low, query, 0.0).astype(jnp.bfloat16)
        key_copies[s].wait()
        scores = lax.dot_general(
            query, keys_vm[s], (((1,), (1,)), ((), ())), preferred_element_type=jnp.float32
        )
        stay, take = [], []
        for b in range(BLOCKS):
            score = scores[:, b * LANES : (b + 1) * LANES] * HD ** (-0.5) - offset
            live = lane + b * LANES < lengths[s]
            tail = jnp.log1p(jnp.exp(-jnp.abs(score)))
            stay.append(jnp.where(live, jnp.minimum(-score, 0.0) - tail, 0.0))
            take.append(jnp.where(live, jnp.minimum(score, 0.0) - tail, -jnp.inf))
        stays.append(stay)
        takes.append(take)

    rest = jnp.concatenate([stays[s][b] for b in range(BLOCKS) for s in range(seqs)], axis=0)
    sums = jnp.zeros((BLOCKS * seqs * H, 2 * LANES), jnp.float32)
    for _ in range(3):
        part = rest.astype(jnp.bfloat16)
        sums = sums + jnp.dot(part, later, preferred_element_type=jnp.float32)
        rest = rest - part.astype(jnp.float32)

    weights = [[None] * BLOCKS for _ in range(seqs)]
    for s in range(seqs):
        beyond = jnp.zeros((H, LANES), jnp.float32)
        for b in reversed(range(BLOCKS)):
            at = (b * seqs + s) * H
            after = sums[at : at + H, :LANES] + beyond
            weights[s][b] = jnp.exp(takes[s][b] + after)
            beyond = beyond + sums[at : at + H, LANES:]

    for s in range(seqs):
        stick = jnp.concatenate(weights[s], axis=1).astype(jnp.bfloat16)
        value_copies[s].wait()
        mixed = jnp.dot(stick, values_vm[s], preferred_element_type=jnp.float32)
        mixed = jnp.where(low, mixed, pltpu.roll(mixed, H // KVH, 0))
        for h in range(H // KVH):
            reads[s : s + 1, h * LANES : (h + 1) * LANES] = mixed[h : h + 1, :]
    done = reads[0:seqs, :].astype(jnp.bfloat16)
    for d in range(out.shape[0]):
        out[d] = done
    for copy in pack_copies:
        copy.wait()


def stick_read(queries, keys, values, lengths, offsets, gate, up, down, copies):
    seqs = queries.shape[0]
    wide, hidden = gate.shape[1], gate.shape[2]
    anywhere = pl.BlockSpec(memory_space=pl.ANY)
    scalars = pl.BlockSpec(memory_space=pltpu.SMEM)
    vector = pl.BlockSpec(memory_space=pltpu.VMEM)
    return pl.pallas_call(
        stick_kernel,
        out_shape=(
            jax.ShapeDtypeStruct((copies, seqs, H * HD), jnp.bfloat16),
            jax.ShapeDtypeStruct((3 * wide, hidden), jnp.bfloat16),
        ),
        in_specs=[scalars, scalars, vector] + [anywhere] * 5,
        out_specs=(vector, anywhere),
        scratch_shapes=[
            pltpu.VMEM(keys.shape, jnp.bfloat16),
            pltpu.VMEM(values.shape, jnp.bfloat16),
            pltpu.VMEM((8, H * HD), jnp.float32),
            pltpu.SemaphoreType.DMA((seqs,)),
            pltpu.SemaphoreType.DMA((seqs,)),
            pltpu.SemaphoreType.DMA((2 + wide // LANES,)),
        ],
        name="stick",
    )(lengths, offsets, queries, keys, values, gate, up, down)


def expert_kernel(rows, gate, up, down, extra, out):
    wide, hidden = gate.shape[1], gate.shape[2]

    def half(gate_part, up_part):
        gated = jnp.dot(rows[...], gate_part, preferred_element_type=jnp.float32)
        upped = jnp.dot(rows[...], up_part, preferred_element_type=jnp.float32)
        return (gated / (1.0 + jnp.exp(-gated)) * upped).astype(jnp.bfloat16)

    own = half(gate[0], up[0])
    other = half(extra[0:wide], extra[wide : 2 * wide])
    for j in range(wide // LANES):
        at = 2 * wide + j * hidden
        piece = jnp.dot(
            own, down[0, :, j * LANES : (j + 1) * LANES], preferred_element_type=jnp.float32
        ) + jnp.dot(other, extra[at : at + hidden], preferred_element_type=jnp.float32)
        out[:, j * LANES : (j + 1) * LANES] = piece.astype(jnp.bfloat16)


def run_expert(rows, gate, up, down, extra):
    return pl.pallas_call(
        expert_kernel,
        out_shape=jax.ShapeDtypeStruct(rows.shape, jnp.bfloat16),
        in_specs=[pl.BlockSpec(memory_space=pltpu.VMEM)] * 5,
        out_specs=pl.BlockSpec(memory_space=pltpu.VMEM),
        name="expert",
    )(rows, gate, up, down, extra)


def exchanged(blocks, axis):
    return lax.all_to_all(blocks, axis, split_axis=0, concat_axis=0, tiled=True)


def moments(values, entries):
    centre = jnp.sum(values, axis=1, keepdims=True) / entries
    spread = jnp.sum(values * values, axis=1, keepdims=True) / entries - centre * centre
    return centre, lax.rsqrt(spread + EPSILON)


def body(
    residual_in,
    queries,
    cache_keys,
    cache_values,
    lengths,
    stick_offset,
    out_weight,
    norm1_gain,
    norm1_bias,
    routes,
    route_weights,
    expert_gate,
    expert_up,
    expert_down,
    shared_gate,
    shared_up,
    shared_down,
    norm2_gain,
    norm2_bias,
):
    peers = lax.axis_size("tp")
    experts = lax.axis_size("ep")
    place = lax.axis_index("tp")
    rows, columns = residual_in.shape
    wide = columns * peers
    mine = place % 2

    mixed, packed = stick_read(
        queries, cache_keys, cache_values, lengths, stick_offset,
        expert_gate, expert_up, expert_down, peers,
    )
    reads = exchanged(mixed, "tp").reshape(rows, H * HD)

    chosen = routes.reshape(-1)
    order = jnp.arange(chosen.shape[0])
    earlier = (chosen[:, None] == chosen[None, :]) & (order[None, :] < order[:, None])
    slots = jnp.sum(earlier.astype(jnp.int32), axis=1).reshape(routes.shape)
    target = jnp.where(slots == mine, routes, -1)
    picks = target[:, :, None] == jnp.arange(experts)[None, None, :]
    dispatch = jnp.sum(picks.astype(jnp.float32), axis=1).astype(jnp.bfloat16)
    combine = jnp.sum(jnp.where(picks, route_weights[:, :, None], 0.0), axis=1)

    weight = out_weight.reshape(KVH, H // KVH, HD, columns).swapaxes(0, 1)
    attended = jnp.dot(
        reads, weight.reshape(H * HD, columns), preferred_element_type=jnp.float32
    )
    before = RESIDUAL_SCALE * residual_in.astype(jnp.float32) + attended
    sent = jnp.concatenate([before, norm1_gain[None], norm1_bias[None]], axis=0)
    got = exchanged(jnp.broadcast_to(sent, (peers, *sent.shape)), "tp")
    got = got.swapaxes(0, 1).reshape(rows + 2, wide)
    widened = got[:rows]
    centre, scale = moments(widened, wide)
    whole = (widened - centre) * scale * got[rows] + got[rows + 1]
    whole = whole.astype(jnp.bfloat16)

    swaps = [(i, i ^ 1) for i in range(peers)]
    extra = lax.ppermute(packed, "tp", swaps)

    parcel = jnp.einsum("se,sd->ed", dispatch, whole, preferred_element_type=jnp.float32)
    parcel = parcel.astype(jnp.bfloat16).reshape(experts, wide // LANES, LANES)
    arrived = exchanged(parcel, "ep").reshape(experts, wide)
    produced = run_expert(arrived, expert_gate, expert_up, expert_down, extra)
    returned = exchanged(produced.reshape(experts, wide // LANES, LANES), "ep")
    routed = jnp.dot(
        combine,
        returned.reshape(experts, wide).astype(jnp.float32),
        precision=lax.Precision.HIGHEST,
    )
    shared_hidden = (
        jax.nn.silu(jnp.dot(whole, shared_gate, preferred_element_type=jnp.float32))
        * jnp.dot(whole, shared_up, preferred_element_type=jnp.float32)
    ).astype(jnp.bfloat16)
    shared = jnp.dot(shared_hidden, shared_down, preferred_element_type=jnp.float32)
    partial = (routed + shared).astype(jnp.bfloat16)
    partials = exchanged(jnp.broadcast_to(partial, (peers, *partial.shape)), "tp")
    after = RESIDUAL_SCALE * whole.astype(jnp.float32) + jnp.sum(
        partials.astype(jnp.float32), axis=0
    )
    centre, scale = moments(after, wide)
    own = lax.dynamic_slice_in_dim(after, place * columns, columns, 1)
    return ((own - centre) * scale * norm2_gain + norm2_bias).astype(jnp.bfloat16)


def solution(mesh):
    in_specs = (
        P("ep", "tp"),
        P(("ep", "tp"), None),
        P(("ep", "tp"), None, None),
        P(("ep", "tp"), None, None),
        P(("ep", "tp")),
        P(),
        P(None, "tp"),
        P("tp"),
        P("tp"),
        P("ep", None),
        P("ep", None),
        P("ep", None, "tp"),
        P("ep", None, "tp"),
        P("ep", "tp", None),
        P(None, "tp"),
        P(None, "tp"),
        P("tp", None),
        P("tp"),
        P("tp"),
    )
    out_specs = P("ep", "tp")
    return jax.shard_map(body, mesh=mesh, in_specs=in_specs, out_specs=out_specs, check_vma=False)
```

```python
import functools

import jax
import jax.numpy as jnp
from jax import lax
from jax.experimental import pallas as pl
from jax.experimental.pallas import tpu as pltpu
from jax.sharding import PartitionSpec as P

H = 8
HD = 64
KVH = 2
CACHE = 1024
TOPK = 6
LANES = 128
BLOCKS = CACHE // LANES
PADDED = 8
GROUP = 24
GRANT = pltpu.CompilerParams(vmem_limit_bytes=12 << 20)

RESIDUAL_SCALE = 2.0**0.25
EPSILON = 1e-05


def stick_kernel(
    lengths, offsets, queries, keys, values, gate, up, down,
    out, packed, keys_vm, values_vm, reads, key_sems, value_sems, pack_sems,
):
    seqs = queries.shape[0]
    wide, hidden = gate.shape[1], gate.shape[2]
    key_copies = [
        pltpu.make_async_copy(keys.at[s], keys_vm.at[s], key_sems.at[s]) for s in range(seqs)
    ]
    value_copies = [
        pltpu.make_async_copy(values.at[s], values_vm.at[s], value_sems.at[s])
        for s in range(seqs)
    ]
    pieces = [(gate.at[0], 0, wide), (up.at[0], wide, wide)]
    for j in range(wide // LANES):
        piece = down.at[0, :, pl.ds(j * LANES, LANES)]
        pieces.append((piece, 2 * wide + j * hidden, hidden))
    pack_copies = [
        pltpu.make_async_copy(piece, packed.at[pl.ds(at, rows)], pack_sems.at[i])
        for i, (piece, at, rows) in enumerate(pieces)
    ]
    for copy in key_copies + value_copies + pack_copies:
        copy.start()

    row = lax.broadcasted_iota(jnp.int32, (H, LANES), 0)
    lane = lax.broadcasted_iota(jnp.int32, (H, LANES), 1)
    low = lane < HD
    first = row < H // KVH
    offset = jnp.zeros((H, LANES), jnp.float32)
    for h in range(H):
        offset = jnp.where(row == h, offsets[h], offset)
    wide_q = queries[...].astype(jnp.float32)
    place = lax.broadcasted_iota(jnp.int32, (LANES, 2 * LANES), 0)
    column = lax.broadcasted_iota(jnp.int32, (LANES, 2 * LANES), 1)
    later = jnp.where((place > column) | (column >= LANES), 1.0, 0.0).astype(jnp.bfloat16)

    stays, takes = [], []
    for s in range(seqs):
        query = jnp.zeros((H, LANES), jnp.float32)
        for h in range(H):
            pair = lax.slice(wide_q, (s, h // 2 * LANES), (s + 1, (h // 2 + 1) * LANES))
            both = jnp.broadcast_to(pair, (H, LANES))
            if h % 2 != h // (H // KVH):
                both = pltpu.roll(both, HD, 1)
            query = jnp.where(row == h, both, query)
        query = jnp.where(first == low, query, 0.0).astype(jnp.bfloat16)
        key_copies[s].wait()
        scores = lax.dot_general(
            query, keys_vm[s], (((1,), (1,)), ((), ())), preferred_element_type=jnp.float32
        )
        stay, take = [], []
        for b in range(BLOCKS):
            score = scores[:, b * LANES : (b + 1) * LANES] * HD ** (-0.5) - offset
            live = lane + b * LANES < lengths[s]
            tail = jnp.log1p(jnp.exp(-jnp.abs(score)))
            stay.append(jnp.where(live, jnp.minimum(-score, 0.0) - tail, 0.0))
            take.append(jnp.where(live, jnp.minimum(score, 0.0) - tail, -jnp.inf))
        stays.append(stay)
        takes.append(take)

    rest = jnp.concatenate([stays[s][b] for b in range(BLOCKS) for s in range(seqs)], axis=0)
    sums = jnp.zeros((BLOCKS * seqs * H, 2 * LANES), jnp.float32)
    for _ in range(3):
        part = rest.astype(jnp.bfloat16)
        sums = sums + jnp.dot(part, later, preferred_element_type=jnp.float32)
        rest = rest - part.astype(jnp.float32)

    weights = [[None] * BLOCKS for _ in range(seqs)]
    for s in range(seqs):
        beyond = jnp.zeros((H, LANES), jnp.float32)
        for b in reversed(range(BLOCKS)):
            at = (b * seqs + s) * H
            after = sums[at : at + H, :LANES] + beyond
            weights[s][b] = jnp.exp(takes[s][b] + after)
            beyond = beyond + sums[at : at + H, LANES:]

    for s in range(seqs):
        stick = jnp.concatenate(weights[s], axis=1).astype(jnp.bfloat16)
        value_copies[s].wait()
        mixed = jnp.dot(stick, values_vm[s], preferred_element_type=jnp.float32)
        mixed = jnp.where(low, mixed, pltpu.roll(mixed, H // KVH, 0))
        for h in range(H // KVH):
            reads[s : s + 1, h * LANES : (h + 1) * LANES] = mixed[h : h + 1, :]
    reads[seqs:, :] = jnp.zeros((reads.shape[0] - seqs, H * HD), jnp.float32)
    done = reads[...].astype(jnp.bfloat16)
    for d in range(out.shape[0]):
        out[d] = done
    for copy in pack_copies:
        copy.wait()


def stick_read(queries, keys, values, lengths, offsets, gate, up, down, copies):
    seqs = queries.shape[0]
    wide, hidden = gate.shape[1], gate.shape[2]
    anywhere = pl.BlockSpec(memory_space=pltpu.HBM)
    scalars = pl.BlockSpec(memory_space=pltpu.SMEM)
    vector = pl.BlockSpec(memory_space=pltpu.VMEM)
    return pl.pallas_call(
        stick_kernel,
        out_shape=(
            jax.ShapeDtypeStruct((copies, PADDED, H * HD), jnp.bfloat16),
            jax.ShapeDtypeStruct((3 * wide, hidden), jnp.bfloat16),
        ),
        in_specs=[scalars, scalars, vector] + [anywhere] * 5,
        out_specs=(vector, vector),
        scratch_shapes=[
            pltpu.VMEM(keys.shape, jnp.bfloat16),
            pltpu.VMEM(values.shape, jnp.bfloat16),
            pltpu.VMEM((PADDED, H * HD), jnp.float32),
            pltpu.SemaphoreType.DMA((seqs,)),
            pltpu.SemaphoreType.DMA((seqs,)),
            pltpu.SemaphoreType.DMA((2 + wide // LANES,)),
        ],
        compiler_params=GRANT,
        name="stick",
    )(*(
        pltpu.with_memory_space_constraint(x, pltpu.HBM)
        for x in (lengths, offsets, queries, keys, values, gate, up, down)
    ))


def project_kernel(reads, weight, residual, gain, bias, out):
    sources, seqs = out.shape[0], residual.shape[0] // out.shape[0]
    rows, columns = residual.shape
    token = lax.broadcasted_iota(jnp.int32, (GROUP, reads.shape[0]), 0)
    arrived = lax.broadcasted_iota(jnp.int32, (GROUP, reads.shape[0]), 1)
    held = jnp.zeros((GROUP, reads.shape[0]), jnp.bool_)
    for t in range(sources):
        inside = (token >= t * seqs) & (token < (t + 1) * seqs)
        held = held | (inside & (arrived == token + t * (PADDED - seqs)))
    held = jnp.where(held, 1.0, 0.0).astype(jnp.bfloat16)
    mixed = jnp.dot(held, reads[...], preferred_element_type=jnp.float32).astype(jnp.bfloat16)
    pairs = H // KVH
    attended = jnp.zeros((GROUP, columns), jnp.float32)
    for h in range(pairs):
        part = jnp.concatenate(
            [weight[h * HD : (h + 1) * HD], weight[(pairs + h) * HD : (pairs + h + 1) * HD]], axis=0
        )
        attended = attended + jnp.dot(
            mixed[:, h * LANES : (h + 1) * LANES], part, preferred_element_type=jnp.float32
        )
    before = RESIDUAL_SCALE * residual[...].astype(jnp.float32) + attended[0:rows]
    rest = jnp.zeros((GROUP - rows - 2, columns), jnp.float32)
    for d in range(sources):
        out[d, 0:rows] = before
        out[d, rows : rows + 1] = gain[...]
        out[d, rows + 1 : rows + 2] = bias[...]
        out[d, rows + 2 :] = rest


def project(reads, weight, residual, gain, bias, copies):
    columns = weight.shape[1]
    vector = pl.BlockSpec(memory_space=pltpu.VMEM)
    return pl.pallas_call(
        project_kernel,
        out_shape=jax.ShapeDtypeStruct((copies, GROUP, columns), jnp.float32),
        in_specs=[vector] * 5,
        out_specs=vector,
        compiler_params=GRANT,
        name="project",
    )(reads, weight, residual, gain.reshape(1, -1), bias.reshape(1, -1))


def row_moments(blocks, entries):
    total = blocks[0]
    squares = blocks[0] * blocks[0]
    for block in blocks[1:]:
        total = total + block
        squares = squares + block * block
    centre = jnp.sum(total, axis=1, keepdims=True) / entries
    spread = jnp.sum(squares, axis=1, keepdims=True) / entries - centre * centre
    return centre, lax.rsqrt(spread + EPSILON)


def norm_kernel(rows, got, dispatch, whole, parcel):
    blocks = []
    for t in range(got.shape[0]):
        for j in range(got.shape[2] // LANES):
            blocks.append(got[t, :, j * LANES : (j + 1) * LANES])
    centre, scale = row_moments(blocks, len(blocks) * LANES)
    normed = []
    for j, block in enumerate(blocks):
        value = (block - centre) * scale * block[rows : rows + 1] + block[rows + 1 : rows + 2]
        normed.append(value)
        whole[:, j * LANES : (j + 1) * LANES] = value.astype(jnp.bfloat16)
    stacked = jnp.concatenate(normed, axis=0).astype(jnp.bfloat16)
    parcel[...] = jnp.dot(
        dispatch[...], stacked, preferred_element_type=jnp.float32
    ).astype(jnp.bfloat16)


def normalize_and_pick(got, dispatch, rows):
    wide = got.shape[0] * got.shape[2]
    vector = pl.BlockSpec(memory_space=pltpu.VMEM)
    return pl.pallas_call(
        functools.partial(norm_kernel, rows),
        out_shape=(
            jax.ShapeDtypeStruct((GROUP, wide), jnp.bfloat16),
            jax.ShapeDtypeStruct((dispatch.shape[0], LANES), jnp.bfloat16),
        ),
        in_specs=[vector] * 2,
        out_specs=(vector, vector),
        compiler_params=GRANT,
        name="norm",
    )(got, dispatch)


def expert_kernel(rows, packed, side, out, turned):
    count, blocks = turned.shape[0], turned.shape[1]
    wide, hidden = blocks * LANES, packed.shape[1]
    turned[...] = rows[...].astype(jnp.float32).reshape(turned.shape)
    features = jnp.concatenate(
        [turned[:, j, :].astype(jnp.bfloat16) for j in range(blocks)], axis=1
    )

    def silu_times(weights):
        gated = jnp.dot(features, weights[0:wide], preferred_element_type=jnp.float32)
        upped = jnp.dot(features, weights[wide : 2 * wide], preferred_element_type=jnp.float32)
        return (gated / (1.0 + jnp.exp(-gated)) * upped).astype(jnp.bfloat16)

    own = silu_times(packed)
    other = silu_times(side)
    for j in range(blocks):
        at = 2 * wide + j * hidden
        turned[:, j, :] = jnp.dot(
            own, packed[at : at + hidden], preferred_element_type=jnp.float32
        ) + jnp.dot(other, side[at : at + hidden], preferred_element_type=jnp.float32)
    out[...] = turned[...].reshape(out.shape).astype(jnp.bfloat16)


def run_expert(rows, packed, side, count):
    blocks = rows.shape[0] // count
    vector = pl.BlockSpec(memory_space=pltpu.VMEM)
    return pl.pallas_call(
        expert_kernel,
        out_shape=jax.ShapeDtypeStruct(rows.shape, jnp.bfloat16),
        in_specs=[vector] * 3,
        out_specs=vector,
        scratch_shapes=[pltpu.VMEM((count, blocks, LANES), jnp.float32)],
        compiler_params=GRANT,
        name="expert",
    )(rows, packed, side)


def combine_kernel(high, low, returned, shared, out):
    total = high.shape[0]
    sums = jnp.dot(high[...], returned[...], preferred_element_type=jnp.float32)
    sums = sums + jnp.dot(low[...], returned[...], preferred_element_type=jnp.float32)
    for j in range(total // GROUP):
        at = slice(j * LANES, (j + 1) * LANES)
        piece = (sums[j * GROUP : (j + 1) * GROUP] + shared[:, at]).astype(jnp.bfloat16)
        for d in range(out.shape[0]):
            out[d, :, at] = piece


def combine_parts(combine, returned, shared, copies):
    vector = pl.BlockSpec(memory_space=pltpu.VMEM)
    return pl.pallas_call(
        combine_kernel,
        out_shape=jax.ShapeDtypeStruct((copies, *shared.shape), jnp.bfloat16),
        in_specs=[vector] * 4,
        out_specs=vector,
        compiler_params=GRANT,
        name="combine",
    )(*combine, returned, shared)


def finish_kernel(place, partials, whole, gain, bias, out, after):
    rows, columns = out.shape
    blocks = []
    for j in range(whole.shape[1] // LANES):
        at = slice(j * LANES, (j + 1) * LANES)
        block = RESIDUAL_SCALE * whole[:, at].astype(jnp.float32)
        for d in range(partials.shape[0]):
            block = block + partials[d, :, at].astype(jnp.float32)
        after[:, at] = block
        blocks.append(block)
    centre, scale = row_moments(blocks, len(blocks) * LANES)
    start = pl.multiple_of(place[0] * columns, columns)
    own = after[:, pl.ds(start, columns)]
    own = (own - centre) * scale * gain[...] + bias[...]
    out[...] = own[0:rows].astype(jnp.bfloat16)


def finish(place, partials, whole, gain, bias, rows):
    vector = pl.BlockSpec(memory_space=pltpu.VMEM)
    return pl.pallas_call(
        finish_kernel,
        out_shape=jax.ShapeDtypeStruct((rows, gain.shape[0]), jnp.bfloat16),
        in_specs=[pl.BlockSpec(memory_space=pltpu.SMEM)] + [vector] * 4,
        out_specs=vector,
        scratch_shapes=[pltpu.VMEM(whole.shape, jnp.float32)],
        compiler_params=GRANT,
        name="finish",
    )(place.reshape(1), partials, whole, gain.reshape(1, -1), bias.reshape(1, -1))


def exchanged(blocks, axis):
    return lax.all_to_all(blocks, axis, split_axis=0, concat_axis=0, tiled=True)


def padded_rows(values, fill):
    short = GROUP - values.shape[0]
    return jnp.pad(values, ((0, short), (0, 0)), constant_values=fill)


def picks_of(routes, route_weights, mine, experts, blocks):
    chosen = routes.reshape(-1)
    order = jnp.arange(chosen.shape[0])
    earlier = (chosen[:, None] == chosen[None, :]) & (order[None, :] < order[:, None])
    slots = jnp.sum(earlier.astype(jnp.int32), axis=1).reshape(routes.shape)
    target = padded_rows(jnp.where(slots == mine, routes, -1), -1)
    weight = padded_rows(route_weights, 0.0)
    target = jnp.tile(target, (blocks, 1))
    weight = jnp.tile(weight, (blocks, 1))
    shape = (blocks * GROUP, experts * blocks)
    block = lax.broadcasted_iota(jnp.int32, shape, 0) // GROUP
    column = lax.broadcasted_iota(jnp.int32, shape, 1)
    expert = jnp.where(column % blocks == block, column // blocks, -2)
    picked = jnp.zeros(shape, jnp.float32)
    combine = jnp.zeros(shape, jnp.float32)
    for k in range(routes.shape[1]):
        hit = target[:, k : k + 1] == expert
        picked = picked + jnp.where(hit, 1.0, 0.0)
        combine = combine + jnp.where(hit, weight[:, k : k + 1], 0.0)
    high = lax.reduce_precision(combine, 8, 7)
    parts = (high.astype(jnp.bfloat16), (combine - high).astype(jnp.bfloat16))
    return picked.T.astype(jnp.bfloat16), parts


def body(
    residual_in,
    queries,
    cache_keys,
    cache_values,
    lengths,
    stick_offset,
    out_weight,
    norm1_gain,
    norm1_bias,
    routes,
    route_weights,
    expert_gate,
    expert_up,
    expert_down,
    shared_gate,
    shared_up,
    shared_down,
    norm2_gain,
    norm2_bias,
):
    peers = lax.axis_size("tp")
    experts = lax.axis_size("ep")
    place = lax.axis_index("tp")
    rows, columns = residual_in.shape
    wide = columns * peers
    blocks = wide // LANES

    mixed, packed = stick_read(
        queries, cache_keys, cache_values, lengths, stick_offset,
        expert_gate, expert_up, expert_down, peers,
    )
    reads = exchanged(mixed, "tp").reshape(peers * PADDED, H * HD)
    dispatch, combine = picks_of(routes, route_weights, place % 2, experts, blocks)
    sent = project(reads, out_weight, residual_in, norm1_gain, norm1_bias, peers)
    got = exchanged(sent, "tp")

    swaps = []
    for e in range(experts):
        for t in range(peers):
            partner = t ^ 1 if e % 2 == 0 else ((t + 1) ^ 1) - 1
            swaps.append((e * peers + t, e * peers + partner % peers))
    side = lax.ppermute(packed, ("ep", "tp"), swaps)

    whole, parcel = normalize_and_pick(got, dispatch, rows)
    arrived = exchanged(parcel.reshape(experts, blocks, LANES), "ep")
    produced = run_expert(arrived.reshape(experts * blocks, LANES), packed, side, experts)
    returned = exchanged(produced.reshape(experts, blocks, LANES), "ep")
    shared_hidden = (
        jax.nn.silu(jnp.dot(whole, shared_gate, preferred_element_type=jnp.float32))
        * jnp.dot(whole, shared_up, preferred_element_type=jnp.float32)
    ).astype(jnp.bfloat16)
    shared = jnp.dot(shared_hidden, shared_down, preferred_element_type=jnp.float32)
    partial = combine_parts(
        combine, returned.reshape(experts * blocks, LANES), shared, peers
    )
    partials = exchanged(partial, "tp")
    return finish(place, partials, whole, norm2_gain, norm2_bias, rows)


def solution(mesh):
    in_specs = (
        P("ep", "tp"),
        P(("ep", "tp"), None),
        P(("ep", "tp"), None, None),
        P(("ep", "tp"), None, None),
        P(("ep", "tp")),
        P(),
        P(None, "tp"),
        P("tp"),
        P("tp"),
        P("ep", None),
        P("ep", None),
        P("ep", None, "tp"),
        P("ep", None, "tp"),
        P("ep", "tp", None),
        P(None, "tp"),
        P(None, "tp"),
        P("tp", None),
        P("tp"),
        P("tp"),
    )
    out_specs = P("ep", "tp")
    return jax.shard_map(body, mesh=mesh, in_specs=in_specs, out_specs=out_specs, check_vma=False)
```

```python
import functools

import jax
import jax.numpy as jnp
from jax import lax
from jax.experimental import pallas as pl
from jax.experimental.pallas import tpu as pltpu
from jax.sharding import PartitionSpec as P


H = 8
HD = 64
KVH = 2
CACHE = 1024
LANES = 128
BLOCKS = CACHE // LANES
PADDED = 8
GROUP = 24
GRANT = pltpu.CompilerParams(vmem_limit_bytes=12 << 20)

RESIDUAL_SCALE = 2.0**0.25
EPSILON = 1e-05


def stick_kernel(
    lengths, offsets, queries, keys, values, gate, up, down,
    out, packed, keys_vm, values_vm, reads, key_sems, value_sems, pack_sems,
):
    seqs = queries.shape[0]
    wide, hidden = gate.shape[1], gate.shape[2]
    key_copies = [
        pltpu.make_async_copy(keys.at[s], keys_vm.at[s], key_sems.at[s]) for s in range(seqs)
    ]
    value_copies = [
        pltpu.make_async_copy(values.at[s], values_vm.at[s], value_sems.at[s])
        for s in range(seqs)
    ]
    pieces = [(gate.at[0], 0, wide), (up.at[0], wide, wide)]
    for j in range(wide // LANES):
        piece = down.at[0, :, pl.ds(j * LANES, LANES)]
        pieces.append((piece, 2 * wide + j * hidden, hidden))
    pack_copies = [
        pltpu.make_async_copy(piece, packed.at[pl.ds(at, rows)], pack_sems.at[i])
        for i, (piece, at, rows) in enumerate(pieces)
    ]
    for copy in key_copies + value_copies + pack_copies:
        copy.start()

    row = lax.broadcasted_iota(jnp.int32, (H, LANES), 0)
    lane = lax.broadcasted_iota(jnp.int32, (H, LANES), 1)
    low = lane < HD
    first = row < H // KVH
    offset = jnp.zeros((H, LANES), jnp.float32)
    for h in range(H):
        offset = jnp.where(row == h, offsets[h], offset)
    wide_q = queries[...].astype(jnp.float32)
    place = lax.broadcasted_iota(jnp.int32, (LANES, 2 * LANES), 0)
    column = lax.broadcasted_iota(jnp.int32, (LANES, 2 * LANES), 1)
    later = jnp.where((place > column) | (column >= LANES), 1.0, 0.0).astype(jnp.bfloat16)

    stays, takes = [], []
    for s in range(seqs):
        query = jnp.zeros((H, LANES), jnp.float32)
        for h in range(H):
            pair = lax.slice(wide_q, (s, h // 2 * LANES), (s + 1, (h // 2 + 1) * LANES))
            both = jnp.broadcast_to(pair, (H, LANES))
            if h % 2 != h // (H // KVH):
                both = pltpu.roll(both, HD, 1)
            query = jnp.where(row == h, both, query)
        query = jnp.where(first == low, query, 0.0).astype(jnp.bfloat16)
        key_copies[s].wait()
        scores = lax.dot_general(
            query, keys_vm[s], (((1,), (1,)), ((), ())), preferred_element_type=jnp.float32
        )
        stay, take = [], []
        for b in range(BLOCKS):
            score = scores[:, b * LANES : (b + 1) * LANES] * HD ** (-0.5) - offset
            live = lane + b * LANES < lengths[s]
            tail = jnp.log1p(jnp.exp(-jnp.abs(score)))
            stay.append(jnp.where(live, jnp.minimum(-score, 0.0) - tail, 0.0))
            take.append(jnp.where(live, jnp.minimum(score, 0.0) - tail, -jnp.inf))
        stays.append(stay)
        takes.append(take)

    rest = jnp.concatenate([stays[s][b] for b in range(BLOCKS) for s in range(seqs)], axis=0)
    sums = jnp.zeros((BLOCKS * seqs * H, 2 * LANES), jnp.float32)
    for _ in range(3):
        part = rest.astype(jnp.bfloat16)
        sums = sums + jnp.dot(part, later, preferred_element_type=jnp.float32)
        rest = rest - part.astype(jnp.float32)

    weights = [[None] * BLOCKS for _ in range(seqs)]
    for s in range(seqs):
        beyond = jnp.zeros((H, LANES), jnp.float32)
        for b in reversed(range(BLOCKS)):
            at = (b * seqs + s) * H
            after = sums[at : at + H, :LANES] + beyond
            weights[s][b] = jnp.exp(takes[s][b] + after)
            beyond = beyond + sums[at : at + H, LANES:]

    for s in range(seqs):
        stick = jnp.concatenate(weights[s], axis=1).astype(jnp.bfloat16)
        value_copies[s].wait()
        mixed = jnp.dot(stick, values_vm[s], preferred_element_type=jnp.float32)
        mixed = jnp.where(low, mixed, pltpu.roll(mixed, H // KVH, 0))
        for h in range(H // KVH):
            reads[s : s + 1, h * LANES : (h + 1) * LANES] = mixed[h : h + 1, :]
    reads[seqs:, :] = jnp.zeros((reads.shape[0] - seqs, H * HD), jnp.float32)
    done = reads[...].astype(jnp.bfloat16)
    for d in range(out.shape[0]):
        out[d] = done
    for copy in pack_copies:
        copy.wait()


def stick_read(queries, keys, values, lengths, offsets, gate, up, down, copies):
    seqs = queries.shape[0]
    wide, hidden = gate.shape[1], gate.shape[2]
    anywhere = pl.BlockSpec(memory_space=pltpu.HBM)
    scalars = pl.BlockSpec(memory_space=pltpu.SMEM)
    vector = pl.BlockSpec(memory_space=pltpu.VMEM)
    return pl.pallas_call(
        stick_kernel,
        out_shape=(
            jax.ShapeDtypeStruct((copies, PADDED, H * HD), jnp.bfloat16),
            jax.ShapeDtypeStruct((3 * wide, hidden), jnp.bfloat16),
        ),
        in_specs=[scalars, scalars, vector] + [anywhere] * 5,
        out_specs=(vector, vector),
        scratch_shapes=[
            pltpu.VMEM(keys.shape, jnp.bfloat16),
            pltpu.VMEM(values.shape, jnp.bfloat16),
            pltpu.VMEM((PADDED, H * HD), jnp.float32),
            pltpu.SemaphoreType.DMA((seqs,)),
            pltpu.SemaphoreType.DMA((seqs,)),
            pltpu.SemaphoreType.DMA((2 + wide // LANES,)),
        ],
        compiler_params=GRANT,
        name="stick",
    )(*(
        pltpu.with_memory_space_constraint(x, pltpu.HBM)
        for x in (lengths, offsets, queries, keys, values, gate, up, down)
    ))


def project_kernel(reads, weight, residual, gain, bias, dispatch, out, parcel):
    rows, columns = residual.shape
    seqs = rows * PADDED // reads.shape[0]
    token = lax.broadcasted_iota(jnp.int32, (GROUP, reads.shape[0]), 0)
    arrived = lax.broadcasted_iota(jnp.int32, (GROUP, reads.shape[0]), 1)
    held = jnp.zeros((GROUP, reads.shape[0]), jnp.float32)
    for t in range(rows // seqs):
        inside = (token >= t * seqs) & (token < (t + 1) * seqs)
        held = jnp.where(inside & (arrived == token + t * (PADDED - seqs)), 1.0, held)
    mixed = jnp.dot(
        held.astype(jnp.bfloat16), reads[...], preferred_element_type=jnp.float32
    ).astype(jnp.bfloat16)
    pairs = H // KVH
    attended = jnp.zeros((GROUP, columns), jnp.float32)
    for h in range(pairs):
        part = jnp.concatenate(
            [weight[h * HD : (h + 1) * HD], weight[(pairs + h) * HD : (pairs + h + 1) * HD]], axis=0
        )
        attended = attended + jnp.dot(
            mixed[:, h * LANES : (h + 1) * LANES], part, preferred_element_type=jnp.float32
        )
    out[0:rows] = RESIDUAL_SCALE * residual[...].astype(jnp.float32) + attended[0:rows]
    out[rows : rows + 1] = gain[...]
    out[rows + 1 : rows + 2] = bias[...]
    out[rows + 2 :] = jnp.zeros((GROUP - rows - 2, columns), jnp.float32)
    stacked = jnp.concatenate(
        [out[:, j * LANES : (j + 1) * LANES] for j in range(columns // LANES)], axis=0
    )
    parcel[...] = jnp.dot(
        dispatch[...], stacked.astype(jnp.bfloat16), preferred_element_type=jnp.float32
    ).astype(jnp.bfloat16)


def project(reads, weight, residual, gain, bias, dispatch):
    columns = weight.shape[1]
    vector = pl.BlockSpec(memory_space=pltpu.VMEM)
    return pl.pallas_call(
        project_kernel,
        out_shape=(
            jax.ShapeDtypeStruct((GROUP, columns), jnp.float32),
            jax.ShapeDtypeStruct((dispatch.shape[0], LANES), jnp.bfloat16),
        ),
        in_specs=[vector] * 6,
        out_specs=(vector, vector),
        compiler_params=GRANT,
        name="project",
    )(reads, weight, residual, gain.reshape(1, -1), bias.reshape(1, -1), dispatch)


def row_moments(blocks, entries):
    total = blocks[0]
    squares = blocks[0] * blocks[0]
    for block in blocks[1:]:
        total = total + block
        squares = squares + block * block
    centre = jnp.sum(total, axis=1, keepdims=True) / entries
    spread = jnp.sum(squares, axis=1, keepdims=True) / entries - centre * centre
    return centre, lax.rsqrt(spread + EPSILON)


def norm_kernel(rows, order, *refs):
    pieces, (whole, affine) = refs[:-2], refs[-2:]
    columns = pieces[0].shape[1]
    blocks = []
    for piece in pieces:
        for j in range(columns // LANES):
            blocks.append(piece[:, j * LANES : (j + 1) * LANES])
    centre, scale = row_moments(blocks, len(blocks) * LANES)
    for i, piece in enumerate(pieces):
        at = pl.ds(pl.multiple_of(order[i] * columns, columns), columns)
        gain, shift = piece[rows : rows + 1], piece[rows + 1 : rows + 2]
        whole[:, at] = ((piece[...] - centre) * scale * gain + shift).astype(jnp.bfloat16)
        affine[0:1, at] = gain
        affine[1:2, at] = shift


def normalize(pieces, order, rows):
    wide = len(pieces) * pieces[0].shape[1]
    vector = pl.BlockSpec(memory_space=pltpu.VMEM)
    return pl.pallas_call(
        functools.partial(norm_kernel, rows),
        out_shape=(
            jax.ShapeDtypeStruct((GROUP, wide), jnp.bfloat16),
            jax.ShapeDtypeStruct((2, wide), jnp.float32),
        ),
        in_specs=[pl.BlockSpec(memory_space=pltpu.SMEM)] + [vector] * len(pieces),
        out_specs=(vector, vector),
        compiler_params=GRANT,
        name="norm",
    )(order, *pieces)


def expert_kernel(rows, affine, packed, side, out, turned):
    blocks = turned.shape[1]
    wide, hidden = blocks * LANES, packed.shape[1]
    turned[...] = rows[...].astype(jnp.float32).reshape(turned.shape)
    parts = [turned[:, j, :] for j in range(blocks)]
    centre, scale = row_moments(parts, wide)
    features = []
    for j, part in enumerate(parts):
        gain = affine[0:1, j * LANES : (j + 1) * LANES]
        shift = affine[1:2, j * LANES : (j + 1) * LANES]
        features.append(((part - centre) * scale * gain + shift).astype(jnp.bfloat16))
    features = jnp.concatenate(features, axis=1)

    def silu_times(weights):
        gated = jnp.dot(features, weights[0:wide], preferred_element_type=jnp.float32)
        upped = jnp.dot(features, weights[wide : 2 * wide], preferred_element_type=jnp.float32)
        return (gated / (1.0 + jnp.exp(-gated)) * upped).astype(jnp.bfloat16)

    own = silu_times(packed)
    other = silu_times(side)
    for j in range(blocks):
        at = 2 * wide + j * hidden
        turned[:, j, :] = jnp.dot(
            own, packed[at : at + hidden], preferred_element_type=jnp.float32
        ) + jnp.dot(other, side[at : at + hidden], preferred_element_type=jnp.float32)
    out[...] = turned[...].reshape(out.shape).astype(jnp.bfloat16)


def run_expert(rows, affine, packed, side, count):
    blocks = rows.shape[0] // count
    vector = pl.BlockSpec(memory_space=pltpu.VMEM)
    return pl.pallas_call(
        expert_kernel,
        out_shape=jax.ShapeDtypeStruct(rows.shape, jnp.bfloat16),
        in_specs=[vector] * 4,
        out_specs=vector,
        scratch_shapes=[pltpu.VMEM((count, blocks, LANES), jnp.float32)],
        compiler_params=GRANT,
        name="expert",
    )(rows, affine, packed, side)


def combine_kernel(high, low, returned, shared, out):
    total = high.shape[0]
    sums = jnp.dot(high[...], returned[...], preferred_element_type=jnp.float32)
    sums = sums + jnp.dot(low[...], returned[...], preferred_element_type=jnp.float32)
    for j in range(total // GROUP):
        at = slice(j * LANES, (j + 1) * LANES)
        piece = (sums[j * GROUP : (j + 1) * GROUP] + shared[:, at]).astype(jnp.bfloat16)
        for d in range(out.shape[0]):
            out[d, :, at] = piece


def combine_parts(combine, returned, shared, copies):
    vector = pl.BlockSpec(memory_space=pltpu.VMEM)
    return pl.pallas_call(
        combine_kernel,
        out_shape=jax.ShapeDtypeStruct((copies, *shared.shape), jnp.bfloat16),
        in_specs=[vector] * 4,
        out_specs=vector,
        compiler_params=GRANT,
        name="combine",
    )(*combine, returned, shared)


def finish_kernel(place, partials, whole, gain, bias, out, after):
    rows, columns = out.shape
    blocks = []
    for j in range(whole.shape[1] // LANES):
        at = slice(j * LANES, (j + 1) * LANES)
        block = RESIDUAL_SCALE * whole[:, at].astype(jnp.float32)
        for d in range(partials.shape[0]):
            block = block + partials[d, :, at].astype(jnp.float32)
        after[:, at] = block
        blocks.append(block)
    centre, scale = row_moments(blocks, len(blocks) * LANES)
    start = pl.multiple_of(place[0] * columns, columns)
    own = after[:, pl.ds(start, columns)]
    own = (own - centre) * scale * gain[...] + bias[...]
    out[...] = own[0:rows].astype(jnp.bfloat16)


def finish(place, partials, whole, gain, bias, rows):
    vector = pl.BlockSpec(memory_space=pltpu.VMEM)
    return pl.pallas_call(
        finish_kernel,
        out_shape=jax.ShapeDtypeStruct((rows, gain.shape[0]), jnp.bfloat16),
        in_specs=[pl.BlockSpec(memory_space=pltpu.SMEM)] + [vector] * 4,
        out_specs=vector,
        scratch_shapes=[pltpu.VMEM(whole.shape, jnp.float32)],
        compiler_params=GRANT,
        name="finish",
    )(place.reshape(1), partials, whole, gain.reshape(1, -1), bias.reshape(1, -1))


def exchanged(blocks, axis):
    return lax.all_to_all(blocks, axis, split_axis=0, concat_axis=0, tiled=True)


def padded_rows(values, fill):
    short = GROUP - values.shape[0]
    return jnp.pad(values, ((0, short), (0, 0)), constant_values=fill)


def picks_of(routes, route_weights, mine, experts, peers, blocks):
    chosen = routes.reshape(-1)
    order = jnp.arange(chosen.shape[0])
    earlier = (chosen[:, None] == chosen[None, :]) & (order[None, :] < order[:, None])
    slots = jnp.sum(earlier.astype(jnp.int32), axis=1).reshape(routes.shape)
    target = padded_rows(routes * 2 + slots, -1)
    weight = padded_rows(route_weights, 0.0)

    pieces = blocks // peers
    shape = (experts * blocks, pieces * GROUP)
    row = lax.broadcasted_iota(jnp.int32, shape, 0)
    piece = lax.broadcasted_iota(jnp.int32, shape, 1) // GROUP
    wanted = row // blocks * 2 + row // pieces % 2
    wanted = jnp.where(row % pieces == piece, wanted, -2)
    turned = jnp.tile(target.T, (1, pieces))
    picked = jnp.zeros(shape, jnp.float32)
    for k in range(routes.shape[1]):
        picked = picked + jnp.where(turned[k : k + 1] == wanted, 1.0, 0.0)

    target = jnp.tile(target, (blocks, 1))
    weight = jnp.tile(weight, (blocks, 1))
    shape = (blocks * GROUP, experts * blocks)
    block = lax.broadcasted_iota(jnp.int32, shape, 0) // GROUP
    column = lax.broadcasted_iota(jnp.int32, shape, 1)
    wanted = jnp.where(column % blocks == block, column // blocks * 2 + mine, -2)
    combine = jnp.zeros(shape, jnp.float32)
    for k in range(routes.shape[1]):
        hit = target[:, k : k + 1] == wanted
        combine = combine + jnp.where(hit, weight[:, k : k + 1], 0.0)
    high = lax.reduce_precision(combine, 8, 7)
    parts = (high.astype(jnp.bfloat16), (combine - high).astype(jnp.bfloat16))
    return picked.astype(jnp.bfloat16), parts


def body(
    residual_in,
    queries,
    cache_keys,
    cache_values,
    lengths,
    stick_offset,
    out_weight,
    norm1_gain,
    norm1_bias,
    routes,
    route_weights,
    expert_gate,
    expert_up,
    expert_down,
    shared_gate,
    shared_up,
    shared_down,
    norm2_gain,
    norm2_bias,
):
    peers = lax.axis_size("tp")
    experts = lax.axis_size("ep")
    place = lax.axis_index("tp")
    rows, columns = residual_in.shape
    wide = columns * peers
    blocks = wide // LANES

    mixed, packed = stick_read(
        queries, cache_keys, cache_values, lengths, stick_offset,
        expert_gate, expert_up, expert_down, peers,
    )
    reads = exchanged(mixed, "tp").reshape(peers * PADDED, H * HD)
    dispatch, combine = picks_of(routes, route_weights, place % 2, experts, peers, blocks)
    sent, parcel = project(
        reads, out_weight, residual_in, norm1_gain, norm1_bias, dispatch
    )
    parcel = parcel.reshape(experts * peers, blocks // peers, LANES)
    arrived = exchanged(parcel, ("ep", "tp")).reshape(experts * blocks, LANES)

    swaps = []
    for e in range(experts):
        for t in range(peers):
            partner = t ^ 1 if e % 2 == 0 else ((t + 1) ^ 1) - 1
            swaps.append((e * peers + t, e * peers + partner % peers))
    side = lax.ppermute(packed, ("ep", "tp"), swaps)
    pieces = [sent]
    for k in range(1, peers):
        pieces.append(lax.ppermute(sent, "tp", [(i, (i + k) % peers) for i in range(peers)]))
    order = (place - jnp.arange(peers, dtype=jnp.int32)) % peers
    whole, affine = normalize(pieces, order, rows)
    produced = run_expert(arrived, affine, packed, side, experts)
    returned = exchanged(produced.reshape(experts, blocks, LANES), "ep")
    shared_hidden = (
        jax.nn.silu(jnp.dot(whole, shared_gate, preferred_element_type=jnp.float32))
        * jnp.dot(whole, shared_up, preferred_element_type=jnp.float32)
    ).astype(jnp.bfloat16)
    shared = jnp.dot(shared_hidden, shared_down, preferred_element_type=jnp.float32)
    partial = combine_parts(
        combine, returned.reshape(experts * blocks, LANES), shared, peers
    )
    partials = exchanged(partial, "tp")
    return finish(place, partials, whole, norm2_gain, norm2_bias, rows)


def solution(mesh):
    in_specs = (
        P("ep", "tp"),
        P(("ep", "tp"), None),
        P(("ep", "tp"), None, None),
        P(("ep", "tp"), None, None),
        P(("ep", "tp")),
        P(),
        P(None, "tp"),
        P("tp"),
        P("tp"),
        P("ep", None),
        P("ep", None),
        P("ep", None, "tp"),
        P("ep", None, "tp"),
        P("ep", "tp", None),
        P(None, "tp"),
        P(None, "tp"),
        P("tp", None),
        P("tp"),
        P("tp"),
    )
    out_specs = P("ep", "tp")

    return jax.shard_map(body, mesh=mesh, in_specs=in_specs, out_specs=out_specs, check_vma=False)
```

```python
import functools

import jax
import jax.numpy as jnp
from jax import lax
from jax.experimental import pallas as pl
from jax.experimental.pallas import tpu as pltpu
from jax.sharding import PartitionSpec as P


H = 8
HD = 64
KVH = 2
CACHE = 1024
LANES = 128
BLOCKS = CACHE // LANES
PADDED = 8
GROUP = 24
GRANT = pltpu.CompilerParams(vmem_limit_bytes=12 << 20)

RESIDUAL_SCALE = 2.0**0.25
EPSILON = 1e-05


def stick_kernel(
    lengths_at, offsets_at, queries_at, keys, values, gate, up, down,
    out, packed, lengths, offsets, queries, keys_vm, values_vm, reads,
    small_sems, key_sems, value_sems, pack_sems,
):
    seqs = keys.shape[0]
    wide, hidden = gate.shape[1], gate.shape[2]
    key_copies = [
        pltpu.make_async_copy(keys.at[s], keys_vm.at[s], key_sems.at[s]) for s in range(seqs)
    ]
    value_copies = [
        pltpu.make_async_copy(values.at[s], values_vm.at[s], value_sems.at[s])
        for s in range(seqs)
    ]
    pieces = [(gate.at[0], 0, wide), (up.at[0], wide, wide)]
    for j in range(wide // LANES):
        piece = down.at[0, :, pl.ds(j * LANES, LANES)]
        pieces.append((piece, 2 * wide + j * hidden, hidden))
    pack_copies = [
        pltpu.make_async_copy(piece, packed.at[pl.ds(at, rows)], pack_sems.at[i])
        for i, (piece, at, rows) in enumerate(pieces)
    ]
    small_copies = [
        pltpu.make_async_copy(source, target, small_sems.at[i])
        for i, (source, target) in enumerate(
            ((queries_at, queries), (lengths_at, lengths), (offsets_at, offsets))
        )
    ]
    for copy in small_copies + key_copies + value_copies + pack_copies:
        copy.start()
    for copy in small_copies:
        copy.wait()

    row = lax.broadcasted_iota(jnp.int32, (H, LANES), 0)
    lane = lax.broadcasted_iota(jnp.int32, (H, LANES), 1)
    low = lane < HD
    first = row < H // KVH
    offset = jnp.zeros((H, LANES), jnp.float32)
    for h in range(H):
        offset = jnp.where(row == h, offsets[h], offset)
    wide_q = queries[...].astype(jnp.float32)
    place = lax.broadcasted_iota(jnp.int32, (LANES, 2 * LANES), 0)
    column = lax.broadcasted_iota(jnp.int32, (LANES, 2 * LANES), 1)
    later = jnp.where((place > column) | (column >= LANES), 1.0, 0.0).astype(jnp.bfloat16)

    stays, takes = [], []
    for s in range(seqs):
        query = jnp.zeros((H, LANES), jnp.float32)
        for h in range(H):
            pair = lax.slice(wide_q, (s, h // 2 * LANES), (s + 1, (h // 2 + 1) * LANES))
            both = jnp.broadcast_to(pair, (H, LANES))
            if h % 2 != h // (H // KVH):
                both = pltpu.roll(both, HD, 1)
            query = jnp.where(row == h, both, query)
        query = jnp.where(first == low, query, 0.0).astype(jnp.bfloat16)
        key_copies[s].wait()
        scores = lax.dot_general(
            query, keys_vm[s], (((1,), (1,)), ((), ())), preferred_element_type=jnp.float32
        )
        stay, take = [], []
        for b in range(BLOCKS):
            score = scores[:, b * LANES : (b + 1) * LANES] * HD ** (-0.5) - offset
            live = lane + b * LANES < lengths[s]
            tail = jnp.log1p(jnp.exp(-jnp.abs(score)))
            stay.append(jnp.where(live, jnp.minimum(-score, 0.0) - tail, 0.0))
            take.append(jnp.where(live, jnp.minimum(score, 0.0) - tail, -jnp.inf))
        stays.append(stay)
        takes.append(take)

    rest = jnp.concatenate([stays[s][b] for b in range(BLOCKS) for s in range(seqs)], axis=0)
    sums = jnp.zeros((BLOCKS * seqs * H, 2 * LANES), jnp.float32)
    for _ in range(3):
        part = rest.astype(jnp.bfloat16)
        sums = sums + jnp.dot(part, later, preferred_element_type=jnp.float32)
        rest = rest - part.astype(jnp.float32)

    weights = [[None] * BLOCKS for _ in range(seqs)]
    for s in range(seqs):
        beyond = jnp.zeros((H, LANES), jnp.float32)
        for b in reversed(range(BLOCKS)):
            at = (b * seqs + s) * H
            after = sums[at : at + H, :LANES] + beyond
            weights[s][b] = jnp.exp(takes[s][b] + after)
            beyond = beyond + sums[at : at + H, LANES:]

    for first_seq in range(0, seqs, 2):
        pair = range(first_seq, min(first_seq + 2, seqs))
        stick = jnp.concatenate(
            [jnp.concatenate(weights[s], axis=1) for s in pair], axis=0
        ).astype(jnp.bfloat16)
        for s in pair:
            value_copies[s].wait()
        both = jnp.concatenate([values_vm[s] for s in pair], axis=1)
        product = jnp.dot(stick, both, preferred_element_type=jnp.float32)
        for i, s in enumerate(pair):
            mixed = product[i * H : (i + 1) * H, i * LANES : (i + 1) * LANES]
            mixed = jnp.where(low, mixed, pltpu.roll(mixed, H // KVH, 0))
            for h in range(H // KVH):
                reads[s : s + 1, h * LANES : (h + 1) * LANES] = mixed[h : h + 1, :]
    reads[seqs:, :] = jnp.zeros((reads.shape[0] - seqs, H * HD), jnp.float32)
    done = reads[...].astype(jnp.bfloat16)
    for d in range(out.shape[0]):
        out[d] = done
    for copy in pack_copies:
        copy.wait()


def stick_read(queries, keys, values, lengths, offsets, gate, up, down, copies):
    seqs = queries.shape[0]
    wide, hidden = gate.shape[1], gate.shape[2]
    anywhere = pl.BlockSpec(memory_space=pltpu.HBM)
    vector = pl.BlockSpec(memory_space=pltpu.VMEM)
    return pl.pallas_call(
        stick_kernel,
        out_shape=(
            jax.ShapeDtypeStruct((copies, PADDED, H * HD), jnp.bfloat16),
            jax.ShapeDtypeStruct((3 * wide, hidden), jnp.bfloat16),
        ),
        in_specs=[anywhere] * 8,
        out_specs=(vector, vector),
        scratch_shapes=[
            pltpu.SMEM(lengths.shape, jnp.int32),
            pltpu.SMEM(offsets.shape, jnp.float32),
            pltpu.VMEM(queries.shape, jnp.bfloat16),
            pltpu.VMEM(keys.shape, jnp.bfloat16),
            pltpu.VMEM(values.shape, jnp.bfloat16),
            pltpu.VMEM((PADDED, H * HD), jnp.float32),
            pltpu.SemaphoreType.DMA((3,)),
            pltpu.SemaphoreType.DMA((seqs,)),
            pltpu.SemaphoreType.DMA((seqs,)),
            pltpu.SemaphoreType.DMA((2 + wide // LANES,)),
        ],
        compiler_params=GRANT,
        name="stick",
    )(*(
        pltpu.with_memory_space_constraint(x, pltpu.HBM)
        for x in (lengths, offsets, queries, keys, values, gate, up, down)
    ))


def project_kernel(reads, weight, residual, gain, bias, out):
    sources, seqs = out.shape[0], residual.shape[0] // out.shape[0]
    rows, columns = residual.shape
    mixed = reads[...]
    pairs = H // KVH
    parts = []
    for h in range(pairs):
        part = jnp.concatenate(
            [weight[h * HD : (h + 1) * HD], weight[(pairs + h) * HD : (pairs + h + 1) * HD]], axis=0
        )
        parts.append(part)
    attended = jnp.dot(
        mixed, jnp.concatenate(parts, axis=0), preferred_element_type=jnp.float32
    )
    attended = jnp.concatenate(
        [attended[t * PADDED : t * PADDED + seqs] for t in range(sources)], axis=0
    )
    before = RESIDUAL_SCALE * residual[...].astype(jnp.float32) + attended
    rest = jnp.zeros((GROUP - rows - 2, columns), jnp.float32)
    for d in range(sources):
        out[d, 0:rows] = before
        out[d, rows : rows + 1] = gain[...]
        out[d, rows + 1 : rows + 2] = bias[...]
        out[d, rows + 2 :] = rest


def project(reads, weight, residual, gain, bias, copies):
    columns = weight.shape[1]
    vector = pl.BlockSpec(memory_space=pltpu.VMEM)
    return pl.pallas_call(
        project_kernel,
        out_shape=jax.ShapeDtypeStruct((copies, GROUP, columns), jnp.float32),
        in_specs=[vector] * 5,
        out_specs=vector,
        compiler_params=GRANT,
        name="project",
    )(reads, weight, residual, gain.reshape(1, -1), bias.reshape(1, -1))


def row_moments(blocks, entries):
    total = blocks[0]
    squares = blocks[0] * blocks[0]
    for block in blocks[1:]:
        total = total + block
        squares = squares + block * block
    centre = jnp.sum(total, axis=1, keepdims=True) / entries
    spread = jnp.sum(squares, axis=1, keepdims=True) / entries - centre * centre
    return centre, lax.rsqrt(spread + EPSILON)


def norm_kernel(rows, got, dispatch, whole, parcel):
    blocks = []
    for t in range(got.shape[0]):
        for j in range(got.shape[2] // LANES):
            blocks.append(got[t, :, j * LANES : (j + 1) * LANES])
    centre, scale = row_moments(blocks, len(blocks) * LANES)
    normed = [
        ((block - centre) * scale * block[rows : rows + 1] + block[rows + 1 : rows + 2])
        for block in blocks
    ]
    normed = jnp.concatenate(normed, axis=1).astype(jnp.bfloat16)
    whole[...] = normed
    picked = jnp.dot(dispatch[...], normed, preferred_element_type=jnp.float32)
    parcel[...] = picked.astype(jnp.bfloat16).reshape(parcel.shape)


def normalize_and_pick(got, dispatch, rows):
    wide = got.shape[0] * got.shape[2]
    vector = pl.BlockSpec(memory_space=pltpu.VMEM)
    return pl.pallas_call(
        functools.partial(norm_kernel, rows),
        out_shape=(
            jax.ShapeDtypeStruct((GROUP, wide), jnp.bfloat16),
            jax.ShapeDtypeStruct((dispatch.shape[0] * wide // LANES, LANES), jnp.bfloat16),
        ),
        in_specs=[vector] * 2,
        out_specs=(vector, vector),
        compiler_params=GRANT,
        name="norm",
    )(got, dispatch)


def expert_kernel(rows, packed, side, out):
    hidden = packed.shape[1]
    wide = packed.shape[0] // 3
    count = rows.shape[0] * LANES // wide
    features = rows[...].reshape(count, wide)

    def silu_times(weights):
        joined = jnp.concatenate([weights[0:wide], weights[wide : 2 * wide]], axis=1)
        product = jnp.dot(features, joined, preferred_element_type=jnp.float32)
        gated, upped = product[:, :hidden], product[:, hidden:]
        return (gated / (1.0 + jnp.exp(-gated)) * upped).astype(jnp.bfloat16)

    both = jnp.concatenate([silu_times(packed), silu_times(side)], axis=1)
    pieces = []
    for j in range(0, wide // LANES, 2):
        at, past = 2 * wide + j * hidden, 2 * wide + (j + 1) * hidden
        down = jnp.concatenate(
            [
                jnp.concatenate([part[at : at + hidden], part[past : past + hidden]], axis=1)
                for part in (packed, side)
            ],
            axis=0,
        )
        pieces.append(jnp.dot(both, down, preferred_element_type=jnp.float32).astype(jnp.bfloat16))
    out[...] = jnp.concatenate(pieces, axis=1).reshape(out.shape)


def run_expert(rows, packed, side):
    vector = pl.BlockSpec(memory_space=pltpu.VMEM)
    return pl.pallas_call(
        expert_kernel,
        out_shape=jax.ShapeDtypeStruct(rows.shape, jnp.bfloat16),
        in_specs=[vector] * 3,
        out_specs=vector,
        compiler_params=GRANT,
        name="expert",
    )(rows, packed, side)


def combine_kernel(high, low, returned, shared, out):
    wide = shared.shape[1]
    results = returned[...].reshape(returned.shape[0] * LANES // wide, wide)
    sums = jnp.dot(high[...], results, preferred_element_type=jnp.float32)
    sums = sums + jnp.dot(low[...], results, preferred_element_type=jnp.float32)
    sums = (sums + shared[...]).astype(jnp.bfloat16)
    for d in range(out.shape[0]):
        out[d] = sums


def combine_parts(combine, returned, shared, copies):
    vector = pl.BlockSpec(memory_space=pltpu.VMEM)
    return pl.pallas_call(
        combine_kernel,
        out_shape=jax.ShapeDtypeStruct((copies, *shared.shape), jnp.bfloat16),
        in_specs=[vector] * 4,
        out_specs=vector,
        compiler_params=GRANT,
        name="combine",
    )(*combine, returned, shared)


def finish_kernel(partials, whole, gain, bias, out, after):
    rows, columns = out.shape
    blocks = []
    for j in range(whole.shape[1] // LANES):
        at = slice(j * LANES, (j + 1) * LANES)
        block = RESIDUAL_SCALE * whole[:, at].astype(jnp.float32)
        for d in range(partials.shape[0]):
            block = block + partials[d, :, at].astype(jnp.float32)
        after[:, at] = block
        blocks.append(block)
    centre, scale = row_moments(blocks, len(blocks) * LANES)
    start = pl.multiple_of(lax.axis_index("tp") * columns, columns)
    own = after[:, pl.ds(start, columns)]
    own = (own - centre) * scale * gain[...] + bias[...]
    out[...] = own[0:rows].astype(jnp.bfloat16)


def finish(partials, whole, gain, bias, rows):
    vector = pl.BlockSpec(memory_space=pltpu.VMEM)
    return pl.pallas_call(
        finish_kernel,
        out_shape=jax.ShapeDtypeStruct((rows, gain.shape[0]), jnp.bfloat16),
        in_specs=[vector] * 4,
        out_specs=vector,
        scratch_shapes=[pltpu.VMEM(whole.shape, jnp.float32)],
        compiler_params=GRANT,
        name="finish",
    )(partials, whole, gain.reshape(1, -1), bias.reshape(1, -1))


def exchanged(blocks, axis):
    return lax.all_to_all(blocks, axis, split_axis=0, concat_axis=0, tiled=True)


def picks_of(routes, route_weights, mine, experts):
    chosen = routes.reshape(-1)
    order = jnp.arange(chosen.shape[0])
    earlier = (chosen[:, None] == chosen[None, :]) & (order[None, :] < order[:, None])
    slots = jnp.sum(earlier.astype(jnp.int32), axis=1).reshape(routes.shape)
    short = ((0, GROUP - routes.shape[0]), (0, 0))
    target = jnp.pad(jnp.where(slots == mine, routes, -1), short, constant_values=-1)
    weight = jnp.pad(route_weights, short)
    picked = jnp.zeros((GROUP, experts), jnp.float32)
    combine = jnp.zeros((GROUP, experts), jnp.float32)
    for k in range(routes.shape[1]):
        hit = target[:, k : k + 1] == jnp.arange(experts)[None, :]
        picked = picked + jnp.where(hit, 1.0, 0.0)
        combine = combine + jnp.where(hit, weight[:, k : k + 1], 0.0)
    high = lax.reduce_precision(combine, 8, 7)
    parts = (high.astype(jnp.bfloat16), (combine - high).astype(jnp.bfloat16))
    return picked.T.astype(jnp.bfloat16), parts


def body(
    residual_in,
    queries,
    cache_keys,
    cache_values,
    lengths,
    stick_offset,
    out_weight,
    norm1_gain,
    norm1_bias,
    routes,
    route_weights,
    expert_gate,
    expert_up,
    expert_down,
    shared_gate,
    shared_up,
    shared_down,
    norm2_gain,
    norm2_bias,
):
    peers = lax.axis_size("tp")
    experts = lax.axis_size("ep")
    place = lax.axis_index("tp")
    rows, columns = residual_in.shape
    wide = columns * peers
    blocks = wide // LANES

    mixed, packed = stick_read(
        queries, cache_keys, cache_values, lengths, stick_offset,
        expert_gate, expert_up, expert_down, peers,
    )
    reads = exchanged(mixed, "tp").reshape(peers * PADDED, H * HD)
    dispatch, combine = picks_of(routes, route_weights, place % 2, experts)
    sent = project(reads, out_weight, residual_in, norm1_gain, norm1_bias, peers)
    got = exchanged(sent, "tp")

    swaps = []
    for e in range(experts):
        for t in range(peers):
            partner = t ^ 1 if e % 2 == 0 else ((t + 1) ^ 1) - 1
            swaps.append((e * peers + t, e * peers + partner % peers))
    side = lax.ppermute(packed, ("ep", "tp"), swaps)

    whole, parcel = normalize_and_pick(got, dispatch, rows)
    arrived = exchanged(parcel.reshape(experts, blocks, LANES), "ep")
    shared_hidden = (
        jax.nn.silu(jnp.dot(whole, shared_gate, preferred_element_type=jnp.float32))
        * jnp.dot(whole, shared_up, preferred_element_type=jnp.float32)
    ).astype(jnp.bfloat16)
    shared = jnp.dot(shared_hidden, shared_down, preferred_element_type=jnp.float32)
    side, shared, combine = lax.optimization_barrier((side, shared, combine))
    produced = run_expert(arrived.reshape(experts * blocks, LANES), packed, side)
    returned = exchanged(produced.reshape(experts, blocks, LANES), "ep")
    partial = combine_parts(
        combine, returned.reshape(experts * blocks, LANES), shared, peers
    )
    partials = exchanged(partial, "tp")
    return finish(partials, whole, norm2_gain, norm2_bias, rows)


def solution(mesh):
    in_specs = (
        P("ep", "tp"),
        P(("ep", "tp"), None),
        P(("ep", "tp"), None, None),
        P(("ep", "tp"), None, None),
        P(("ep", "tp")),
        P(),
        P(None, "tp"),
        P("tp"),
        P("tp"),
        P("ep", None),
        P("ep", None),
        P("ep", None, "tp"),
        P("ep", None, "tp"),
        P("ep", "tp", None),
        P(None, "tp"),
        P(None, "tp"),
        P("tp", None),
        P("tp"),
        P("tp"),
    )
    out_specs = P("ep", "tp")

    return jax.shard_map(body, mesh=mesh, in_specs=in_specs, out_specs=out_specs, check_vma=False)
```

```python
import functools

import jax
import jax.numpy as jnp
from jax import lax
from jax.experimental import pallas as pl
from jax.experimental.pallas import tpu as pltpu
from jax.sharding import PartitionSpec as P


H = 8
HD = 64
KVH = 2
CACHE = 1024
LANES = 128
BLOCKS = CACHE // LANES
PADDED = 8
GROUP = 24
GRANT = pltpu.CompilerParams(vmem_limit_bytes=12 << 20)

RESIDUAL_SCALE = 2.0**0.25
EPSILON = 1e-05


def route_tables(routes, shares, chosen, share, dispatch, high, low):
    picks, tokens = routes.shape
    chosen[...] = jnp.full(chosen.shape, -1, jnp.int32)
    share[...] = jnp.zeros(share.shape, jnp.float32)
    chosen[0:picks, 0:tokens] = routes[...]
    share[0:picks, 0:tokens] = shares[...]
    shape = (dispatch.shape[0], LANES)
    expert = lax.broadcasted_iota(jnp.int32, shape, 0)
    hits = [chosen[k : k + 1, :] == expert for k in range(picks)]
    named = jnp.zeros(shape, jnp.float32)
    for hit in hits:
        named = jnp.where(hit, 1.0, named)
    before = lax.broadcasted_iota(jnp.int32, (LANES, LANES), 0)
    token = lax.broadcasted_iota(jnp.int32, (LANES, LANES), 1)
    sooner = jnp.where(before < token, 1.0, 0.0).astype(jnp.bfloat16)
    slot = jnp.dot(named.astype(jnp.bfloat16), sooner, preferred_element_type=jnp.float32)
    mine = (lax.axis_index("tp") % 2).astype(jnp.float32)
    held = slot == mine
    dispatch[...] = jnp.where(held, named, 0.0).astype(jnp.bfloat16)
    weight = jnp.zeros(shape, jnp.float32)
    for k, hit in enumerate(hits):
        weight = jnp.where(hit & held, share[k : k + 1, :], weight)
    weight = weight.T[0 : high.shape[0]]
    upper = weight.astype(jnp.bfloat16)
    high[...] = upper
    low[...] = (weight - upper.astype(jnp.float32)).astype(jnp.bfloat16)


def stick_kernel(
    lengths_at, offsets_at, queries_at, routes_at, shares_at, keys, values, gate, up, down,
    out, packed, dispatch, high, low,
    lengths, offsets, queries, routes, shares, chosen, share, keys_vm, values_vm, reads,
    small_sems, key_sems, value_sems, pack_sems,
):
    seqs = keys.shape[0]
    wide, hidden = gate.shape[1], gate.shape[2]
    key_copies = [
        pltpu.make_async_copy(keys.at[s], keys_vm.at[s], key_sems.at[s]) for s in range(seqs)
    ]
    value_copies = [
        pltpu.make_async_copy(values.at[s], values_vm.at[s], value_sems.at[s])
        for s in range(seqs)
    ]
    pieces = [(gate.at[0], 0, wide), (up.at[0], wide, wide)]
    for j in range(wide // LANES):
        piece = down.at[0, :, pl.ds(j * LANES, LANES)]
        pieces.append((piece, 2 * wide + j * hidden, hidden))
    pack_copies = [
        pltpu.make_async_copy(piece, packed.at[pl.ds(at, rows)], pack_sems.at[i])
        for i, (piece, at, rows) in enumerate(pieces)
    ]
    small_copies = [
        pltpu.make_async_copy(source, target, small_sems.at[i])
        for i, (source, target) in enumerate(
            (
                (routes_at, routes),
                (shares_at, shares),
                (queries_at, queries),
                (lengths_at, lengths),
                (offsets_at, offsets),
            )
        )
    ]
    for copy in small_copies + key_copies + value_copies + pack_copies:
        copy.start()
    for copy in small_copies:
        copy.wait()
    route_tables(routes, shares, chosen, share, dispatch, high, low)

    row = lax.broadcasted_iota(jnp.int32, (H, LANES), 0)
    lane = lax.broadcasted_iota(jnp.int32, (H, LANES), 1)
    low = lane < HD
    first = row < H // KVH
    offset = jnp.zeros((H, LANES), jnp.float32)
    for h in range(H):
        offset = jnp.where(row == h, offsets[h], offset)
    wide_q = queries[...].astype(jnp.float32)
    place = lax.broadcasted_iota(jnp.int32, (LANES, 2 * LANES), 0)
    column = lax.broadcasted_iota(jnp.int32, (LANES, 2 * LANES), 1)
    later = jnp.where((place > column) | (column >= LANES), 1.0, 0.0).astype(jnp.bfloat16)

    stays, takes = [], []
    for s in range(seqs):
        query = jnp.zeros((H, LANES), jnp.float32)
        for h in range(H):
            pair = lax.slice(wide_q, (s, h // 2 * LANES), (s + 1, (h // 2 + 1) * LANES))
            both = jnp.broadcast_to(pair, (H, LANES))
            if h % 2 != h // (H // KVH):
                both = pltpu.roll(both, HD, 1)
            query = jnp.where(row == h, both, query)
        query = jnp.where(first == low, query, 0.0).astype(jnp.bfloat16)
        key_copies[s].wait()
        scores = lax.dot_general(
            query, keys_vm[s], (((1,), (1,)), ((), ())), preferred_element_type=jnp.float32
        )
        stay, take = [], []
        for b in range(BLOCKS):
            score = scores[:, b * LANES : (b + 1) * LANES] * HD ** (-0.5) - offset
            live = lane + b * LANES < lengths[s]
            tail = jnp.log1p(jnp.exp(-jnp.abs(score)))
            stay.append(jnp.where(live, jnp.minimum(-score, 0.0) - tail, 0.0))
            take.append(jnp.where(live, jnp.minimum(score, 0.0) - tail, -jnp.inf))
        stays.append(stay)
        takes.append(take)

    rest = jnp.concatenate([stays[s][b] for b in range(BLOCKS) for s in range(seqs)], axis=0)
    sums = jnp.zeros((BLOCKS * seqs * H, 2 * LANES), jnp.float32)
    for _ in range(3):
        part = rest.astype(jnp.bfloat16)
        sums = sums + jnp.dot(part, later, preferred_element_type=jnp.float32)
        rest = rest - part.astype(jnp.float32)

    weights = [[None] * BLOCKS for _ in range(seqs)]
    for s in range(seqs):
        beyond = jnp.zeros((H, LANES), jnp.float32)
        for b in reversed(range(BLOCKS)):
            at = (b * seqs + s) * H
            after = sums[at : at + H, :LANES] + beyond
            weights[s][b] = jnp.exp(takes[s][b] + after)
            beyond = beyond + sums[at : at + H, LANES:]

    for first_seq in range(0, seqs, 2):
        pair = range(first_seq, min(first_seq + 2, seqs))
        stick = jnp.concatenate(
            [jnp.concatenate(weights[s], axis=1) for s in pair], axis=0
        ).astype(jnp.bfloat16)
        for s in pair:
            value_copies[s].wait()
        both = jnp.concatenate([values_vm[s] for s in pair], axis=1)
        product = jnp.dot(stick, both, preferred_element_type=jnp.float32)
        for i, s in enumerate(pair):
            mixed = product[i * H : (i + 1) * H, i * LANES : (i + 1) * LANES]
            mixed = jnp.where(low, mixed, pltpu.roll(mixed, H // KVH, 0))
            for h in range(H // KVH):
                reads[s : s + 1, h * LANES : (h + 1) * LANES] = mixed[h : h + 1, :]
    reads[seqs:, :] = jnp.zeros((reads.shape[0] - seqs, H * HD), jnp.float32)
    done = reads[...].astype(jnp.bfloat16)
    for d in range(out.shape[0]):
        out[d] = done
    for copy in pack_copies:
        copy.wait()


def stick_read(
    queries, keys, values, lengths, offsets, routes, shares, gate, up, down, copies, experts
):
    seqs = queries.shape[0]
    wide, hidden = gate.shape[1], gate.shape[2]
    anywhere = pl.BlockSpec(memory_space=pltpu.HBM)
    vector = pl.BlockSpec(memory_space=pltpu.VMEM)
    return pl.pallas_call(
        stick_kernel,
        out_shape=(
            jax.ShapeDtypeStruct((copies, PADDED, H * HD), jnp.bfloat16),
            jax.ShapeDtypeStruct((3 * wide, hidden), jnp.bfloat16),
            jax.ShapeDtypeStruct((experts, LANES), jnp.bfloat16),
            jax.ShapeDtypeStruct((GROUP, experts), jnp.bfloat16),
            jax.ShapeDtypeStruct((GROUP, experts), jnp.bfloat16),
        ),
        in_specs=[anywhere] * 10,
        out_specs=(vector,) * 5,
        scratch_shapes=[
            pltpu.SMEM(lengths.shape, jnp.int32),
            pltpu.SMEM(offsets.shape, jnp.float32),
            pltpu.VMEM(queries.shape, jnp.bfloat16),
            pltpu.VMEM(routes.shape, jnp.int32),
            pltpu.VMEM(shares.shape, jnp.float32),
            pltpu.VMEM((8, LANES), jnp.int32),
            pltpu.VMEM((8, LANES), jnp.float32),
            pltpu.VMEM(keys.shape, jnp.bfloat16),
            pltpu.VMEM(values.shape, jnp.bfloat16),
            pltpu.VMEM((PADDED, H * HD), jnp.float32),
            pltpu.SemaphoreType.DMA((5,)),
            pltpu.SemaphoreType.DMA((seqs,)),
            pltpu.SemaphoreType.DMA((seqs,)),
            pltpu.SemaphoreType.DMA((2 + wide // LANES,)),
        ],
        compiler_params=GRANT,
        name="stick",
    )(*(
        pltpu.with_memory_space_constraint(x, pltpu.HBM)
        for x in (lengths, offsets, queries, routes, shares, keys, values, gate, up, down)
    ))


def project_kernel(reads, weight, residual, gain, bias, out):
    sources, seqs = out.shape[0], residual.shape[0] // out.shape[0]
    rows, columns = residual.shape
    mixed = reads[...]
    pairs = H // KVH
    parts = []
    for h in range(pairs):
        part = jnp.concatenate(
            [weight[h * HD : (h + 1) * HD], weight[(pairs + h) * HD : (pairs + h + 1) * HD]], axis=0
        )
        parts.append(part)
    attended = jnp.dot(
        mixed, jnp.concatenate(parts, axis=0), preferred_element_type=jnp.float32
    )
    attended = jnp.concatenate(
        [attended[t * PADDED : t * PADDED + seqs] for t in range(sources)], axis=0
    )
    before = RESIDUAL_SCALE * residual[...].astype(jnp.float32) + attended
    rest = jnp.zeros((GROUP - rows - 2, columns), jnp.float32)
    for d in range(sources):
        out[d, 0:rows] = before
        out[d, rows : rows + 1] = gain[...]
        out[d, rows + 1 : rows + 2] = bias[...]
        out[d, rows + 2 :] = rest


def project(reads, weight, residual, gain, bias, copies):
    columns = weight.shape[1]
    vector = pl.BlockSpec(memory_space=pltpu.VMEM)
    return pl.pallas_call(
        project_kernel,
        out_shape=jax.ShapeDtypeStruct((copies, GROUP, columns), jnp.float32),
        in_specs=[vector] * 5,
        out_specs=vector,
        compiler_params=GRANT,
        name="project",
    )(reads, weight, residual, gain.reshape(1, -1), bias.reshape(1, -1))


def row_moments(blocks, entries):
    total = blocks[0]
    squares = blocks[0] * blocks[0]
    for block in blocks[1:]:
        total = total + block
        squares = squares + block * block
    centre = jnp.sum(total, axis=1, keepdims=True) / entries
    spread = jnp.sum(squares, axis=1, keepdims=True) / entries - centre * centre
    return centre, lax.rsqrt(spread + EPSILON)


def norm_kernel(rows, got, dispatch, whole, parcel):
    blocks = []
    for t in range(got.shape[0]):
        for j in range(got.shape[2] // LANES):
            blocks.append(got[t, :, j * LANES : (j + 1) * LANES])
    centre, scale = row_moments(blocks, len(blocks) * LANES)
    normed = [
        ((block - centre) * scale * block[rows : rows + 1] + block[rows + 1 : rows + 2])
        for block in blocks
    ]
    normed = jnp.concatenate(normed, axis=1).astype(jnp.bfloat16)
    whole[...] = normed
    picked = jnp.dot(dispatch[:, 0:GROUP], normed, preferred_element_type=jnp.float32)
    parcel[...] = picked.astype(jnp.bfloat16).reshape(parcel.shape)


def normalize_and_pick(got, dispatch, rows):
    wide = got.shape[0] * got.shape[2]
    vector = pl.BlockSpec(memory_space=pltpu.VMEM)
    return pl.pallas_call(
        functools.partial(norm_kernel, rows),
        out_shape=(
            jax.ShapeDtypeStruct((GROUP, wide), jnp.bfloat16),
            jax.ShapeDtypeStruct((dispatch.shape[0] * wide // LANES, LANES), jnp.bfloat16),
        ),
        in_specs=[vector] * 2,
        out_specs=(vector, vector),
        compiler_params=GRANT,
        name="norm",
    )(got, dispatch)


def expert_kernel(rows, packed, side, out):
    hidden = packed.shape[1]
    wide = packed.shape[0] // 3
    count = rows.shape[0] * LANES // wide
    features = rows[...].reshape(count, wide)

    def silu_times(weights):
        joined = jnp.concatenate([weights[0:wide], weights[wide : 2 * wide]], axis=1)
        product = jnp.dot(features, joined, preferred_element_type=jnp.float32)
        gated, upped = product[:, :hidden], product[:, hidden:]
        return (gated / (1.0 + jnp.exp(-gated)) * upped).astype(jnp.bfloat16)

    both = jnp.concatenate([silu_times(packed), silu_times(side)], axis=1)
    pieces = []
    for j in range(0, wide // LANES, 2):
        at, past = 2 * wide + j * hidden, 2 * wide + (j + 1) * hidden
        down = jnp.concatenate(
            [
                jnp.concatenate([part[at : at + hidden], part[past : past + hidden]], axis=1)
                for part in (packed, side)
            ],
            axis=0,
        )
        pieces.append(jnp.dot(both, down, preferred_element_type=jnp.float32).astype(jnp.bfloat16))
    out[...] = jnp.concatenate(pieces, axis=1).reshape(out.shape)


def run_expert(rows, packed, side):
    vector = pl.BlockSpec(memory_space=pltpu.VMEM)
    return pl.pallas_call(
        expert_kernel,
        out_shape=jax.ShapeDtypeStruct(rows.shape, jnp.bfloat16),
        in_specs=[vector] * 3,
        out_specs=vector,
        compiler_params=GRANT,
        name="expert",
    )(rows, packed, side)


def combine_kernel(high, low, returned, shared, out):
    wide = shared.shape[1]
    results = returned[...].reshape(returned.shape[0] * LANES // wide, wide)
    sums = jnp.dot(high[...], results, preferred_element_type=jnp.float32)
    sums = sums + jnp.dot(low[...], results, preferred_element_type=jnp.float32)
    sums = (sums + shared[...]).astype(jnp.bfloat16)
    for d in range(out.shape[0]):
        out[d] = sums


def combine_parts(combine, returned, shared, copies):
    vector = pl.BlockSpec(memory_space=pltpu.VMEM)
    return pl.pallas_call(
        combine_kernel,
        out_shape=jax.ShapeDtypeStruct((copies, *shared.shape), jnp.bfloat16),
        in_specs=[vector] * 4,
        out_specs=vector,
        compiler_params=GRANT,
        name="combine",
    )(*combine, returned, shared)


def finish_kernel(partials, whole, gain, bias, out, after):
    rows, columns = out.shape
    blocks = []
    for j in range(whole.shape[1] // LANES):
        at = slice(j * LANES, (j + 1) * LANES)
        block = RESIDUAL_SCALE * whole[:, at].astype(jnp.float32)
        for d in range(partials.shape[0]):
            block = block + partials[d, :, at].astype(jnp.float32)
        after[:, at] = block
        blocks.append(block)
    centre, scale = row_moments(blocks, len(blocks) * LANES)
    start = pl.multiple_of(lax.axis_index("tp") * columns, columns)
    own = after[:, pl.ds(start, columns)]
    own = (own - centre) * scale * gain[...] + bias[...]
    out[...] = own[0:rows].astype(jnp.bfloat16)


def finish(partials, whole, gain, bias, rows):
    vector = pl.BlockSpec(memory_space=pltpu.VMEM)
    return pl.pallas_call(
        finish_kernel,
        out_shape=jax.ShapeDtypeStruct((rows, gain.shape[0]), jnp.bfloat16),
        in_specs=[vector] * 4,
        out_specs=vector,
        scratch_shapes=[pltpu.VMEM(whole.shape, jnp.float32)],
        compiler_params=GRANT,
        name="finish",
    )(partials, whole, gain.reshape(1, -1), bias.reshape(1, -1))


def exchanged(blocks, axis):
    return lax.all_to_all(blocks, axis, split_axis=0, concat_axis=0, tiled=True)


def body(
    residual_in,
    queries,
    cache_keys,
    cache_values,
    lengths,
    stick_offset,
    out_weight,
    norm1_gain,
    norm1_bias,
    routes,
    route_weights,
    expert_gate,
    expert_up,
    expert_down,
    shared_gate,
    shared_up,
    shared_down,
    norm2_gain,
    norm2_bias,
):
    peers = lax.axis_size("tp")
    experts = lax.axis_size("ep")
    rows, columns = residual_in.shape
    wide = columns * peers
    blocks = wide // LANES

    mixed, packed, dispatch, high, low = stick_read(
        queries, cache_keys, cache_values, lengths, stick_offset, routes.T, route_weights.T,
        expert_gate, expert_up, expert_down, peers, experts,
    )
    reads = exchanged(mixed, "tp").reshape(peers * PADDED, H * HD)
    sent = project(reads, out_weight, residual_in, norm1_gain, norm1_bias, peers)
    got = exchanged(sent, "tp")

    swaps = []
    for e in range(experts):
        for t in range(peers):
            partner = t ^ 1 if e % 2 == 0 else ((t + 1) ^ 1) - 1
            swaps.append((e * peers + t, e * peers + partner % peers))
    side = lax.ppermute(packed, ("ep", "tp"), swaps)

    whole, parcel = normalize_and_pick(got, dispatch, rows)
    arrived = exchanged(parcel.reshape(experts, blocks, LANES), "ep")
    shared_hidden = (
        jax.nn.silu(jnp.dot(whole, shared_gate, preferred_element_type=jnp.float32))
        * jnp.dot(whole, shared_up, preferred_element_type=jnp.float32)
    ).astype(jnp.bfloat16)
    shared = jnp.dot(shared_hidden, shared_down, preferred_element_type=jnp.float32)
    side, shared = lax.optimization_barrier((side, shared))
    produced = run_expert(arrived.reshape(experts * blocks, LANES), packed, side)
    returned = exchanged(produced.reshape(experts, blocks, LANES), "ep")
    partial = combine_parts(
        (high, low), returned.reshape(experts * blocks, LANES), shared, peers
    )
    partials = exchanged(partial, "tp")
    return finish(partials, whole, norm2_gain, norm2_bias, rows)


def solution(mesh):
    in_specs = (
        P("ep", "tp"),
        P(("ep", "tp"), None),
        P(("ep", "tp"), None, None),
        P(("ep", "tp"), None, None),
        P(("ep", "tp")),
        P(),
        P(None, "tp"),
        P("tp"),
        P("tp"),
        P("ep", None),
        P("ep", None),
        P("ep", None, "tp"),
        P("ep", None, "tp"),
        P("ep", "tp", None),
        P(None, "tp"),
        P(None, "tp"),
        P("tp", None),
        P("tp"),
        P("tp"),
    )
    out_specs = P("ep", "tp")

    return jax.shard_map(body, mesh=mesh, in_specs=in_specs, out_specs=out_specs, check_vma=False)
```

```python
import functools

import jax
import jax.numpy as jnp
from jax import lax
from jax.experimental import pallas as pl
from jax.experimental.pallas import tpu as pltpu
from jax.sharding import PartitionSpec as P


H = 8
HD = 64
KVH = 2
CACHE = 1024
LANES = 128
BLOCKS = CACHE // LANES
PADDED = 8
GROUP = 24
GRANT = pltpu.CompilerParams(vmem_limit_bytes=12 << 20)

RESIDUAL_SCALE = 2.0**0.25
EPSILON = 1e-05


def route_tables(routes, shares, chosen, share, dispatch, high, low):
    picks, tokens = routes.shape
    chosen[...] = jnp.full(chosen.shape, -1, jnp.int32)
    share[...] = jnp.zeros(share.shape, jnp.float32)
    chosen[0:picks, 0:tokens] = routes[...]
    share[0:picks, 0:tokens] = shares[...]
    shape = (dispatch.shape[0], LANES)
    expert = lax.broadcasted_iota(jnp.int32, shape, 0)
    hits = [chosen[k : k + 1, :] == expert for k in range(picks)]
    named = jnp.zeros(shape, jnp.float32)
    for hit in hits:
        named = jnp.where(hit, 1.0, named)
    before = lax.broadcasted_iota(jnp.int32, (LANES, LANES), 0)
    token = lax.broadcasted_iota(jnp.int32, (LANES, LANES), 1)
    sooner = jnp.where(before < token, 1.0, 0.0).astype(jnp.bfloat16)
    slot = jnp.dot(named.astype(jnp.bfloat16), sooner, preferred_element_type=jnp.float32)
    mine = (lax.axis_index("tp") % 2).astype(jnp.float32)
    held = slot == mine
    dispatch[...] = jnp.where(held, named, 0.0).astype(jnp.bfloat16)
    weight = jnp.zeros(shape, jnp.float32)
    for k, hit in enumerate(hits):
        weight = jnp.where(hit & held, share[k : k + 1, :], weight)
    weight = weight.T[0 : high.shape[0]]
    upper = weight.astype(jnp.bfloat16)
    high[...] = upper
    low[...] = (weight - upper.astype(jnp.float32)).astype(jnp.bfloat16)


def stick_kernel(
    lengths_at, offsets_at, queries_at, routes_at, shares_at, keys, values, gate, up, down,
    out, packed, dispatch, high, low,
    lengths, offsets, queries, routes, shares, chosen, share, keys_vm, values_vm, reads,
    small_sems, key_sems, value_sems, pack_sems,
):
    seqs = keys.shape[0]
    wide, hidden = gate.shape[1], gate.shape[2]
    key_copies = [
        pltpu.make_async_copy(keys.at[s], keys_vm.at[s], key_sems.at[s]) for s in range(seqs)
    ]
    value_copies = [
        pltpu.make_async_copy(values.at[s], values_vm.at[s], value_sems.at[s])
        for s in range(seqs)
    ]
    pieces = [(gate.at[0], 0, wide), (up.at[0], wide, wide)]
    for j in range(wide // LANES):
        piece = down.at[0, :, pl.ds(j * LANES, LANES)]
        pieces.append((piece, 2 * wide + j * hidden, hidden))
    pack_copies = [
        pltpu.make_async_copy(piece, packed.at[pl.ds(at, rows)], pack_sems.at[i])
        for i, (piece, at, rows) in enumerate(pieces)
    ]
    small_copies = [
        pltpu.make_async_copy(source, target, small_sems.at[i])
        for i, (source, target) in enumerate(
            (
                (routes_at, routes),
                (shares_at, shares),
                (queries_at, queries),
                (lengths_at, lengths),
                (offsets_at, offsets),
            )
        )
    ]
    for copy in small_copies + key_copies + value_copies:
        copy.start()
    for copy in small_copies:
        copy.wait()
    route_tables(routes, shares, chosen, share, dispatch, high, low)

    row = lax.broadcasted_iota(jnp.int32, (H, LANES), 0)
    lane = lax.broadcasted_iota(jnp.int32, (H, LANES), 1)
    low = lane < HD
    first = row < H // KVH
    offset = jnp.zeros((H, LANES), jnp.float32)
    for h in range(H):
        offset = jnp.where(row == h, offsets[h], offset)
    wide_q = queries[...].astype(jnp.float32)
    place = lax.broadcasted_iota(jnp.int32, (LANES, 2 * LANES), 0)
    column = lax.broadcasted_iota(jnp.int32, (LANES, 2 * LANES), 1)
    later = jnp.where((place > column) | (column >= LANES), 1.0, 0.0).astype(jnp.bfloat16)

    built = []
    for s in range(seqs):
        query = jnp.zeros((H, LANES), jnp.float32)
        for h in range(H):
            pair = lax.slice(wide_q, (s, h // 2 * LANES), (s + 1, (h // 2 + 1) * LANES))
            both = jnp.broadcast_to(pair, (H, LANES))
            if h % 2 != h // (H // KVH):
                both = pltpu.roll(both, HD, 1)
            query = jnp.where(row == h, both, query)
        query = jnp.where(first == low, query, 0.0).astype(jnp.bfloat16)
        built.append(query)
    stays, takes = [], []
    for s in range(seqs):
        if s % 2 == 0:
            pair = range(s, min(s + 2, seqs))
            for p in pair:
                key_copies[p].wait()
            joined = jnp.concatenate([built[p] for p in pair], axis=0)
            keyed = jnp.concatenate([keys_vm[p] for p in pair], axis=0)
            product = lax.dot_general(
                joined, keyed, (((1,), (1,)), ((), ())), preferred_element_type=jnp.float32
            )
        i = s % 2
        scores = product[i * H : (i + 1) * H, i * CACHE : (i + 1) * CACHE]
        stay, take = [], []
        for b in range(BLOCKS):
            score = scores[:, b * LANES : (b + 1) * LANES] * HD ** (-0.5) - offset
            live = lane + b * LANES < lengths[s]
            tail = jnp.log1p(jnp.exp(-jnp.abs(score)))
            stay.append(jnp.where(live, jnp.minimum(-score, 0.0) - tail, 0.0))
            take.append(jnp.where(live, jnp.minimum(score, 0.0) - tail, -jnp.inf))
        stays.append(stay)
        takes.append(take)

    for copy in pack_copies:
        copy.start()
    rest = jnp.concatenate([stays[s][b] for b in range(BLOCKS) for s in range(seqs)], axis=0)
    sums = jnp.zeros((BLOCKS * seqs * H, 2 * LANES), jnp.float32)
    for _ in range(3):
        part = rest.astype(jnp.bfloat16)
        sums = sums + jnp.dot(part, later, preferred_element_type=jnp.float32)
        rest = rest - part.astype(jnp.float32)

    weights = [[None] * BLOCKS for _ in range(seqs)]
    for s in range(seqs):
        beyond = jnp.zeros((H, LANES), jnp.float32)
        for b in reversed(range(BLOCKS)):
            at = (b * seqs + s) * H
            after = sums[at : at + H, :LANES] + beyond
            weights[s][b] = jnp.exp(takes[s][b] + after)
            beyond = beyond + sums[at : at + H, LANES:]

    for first_seq in range(0, seqs, 2):
        pair = range(first_seq, min(first_seq + 2, seqs))
        stick = jnp.concatenate(
            [jnp.concatenate(weights[s], axis=1) for s in pair], axis=0
        ).astype(jnp.bfloat16)
        for s in pair:
            value_copies[s].wait()
        both = jnp.concatenate([values_vm[s] for s in pair], axis=1)
        product = jnp.dot(stick, both, preferred_element_type=jnp.float32)
        for i, s in enumerate(pair):
            mixed = product[i * H : (i + 1) * H, i * LANES : (i + 1) * LANES]
            mixed = jnp.where(low, mixed, pltpu.roll(mixed, H // KVH, 0))
            for h in range(H // KVH):
                reads[s : s + 1, h * LANES : (h + 1) * LANES] = mixed[h : h + 1, :]
    reads[seqs:, :] = jnp.zeros((reads.shape[0] - seqs, H * HD), jnp.float32)
    done = reads[...].astype(jnp.bfloat16)
    for d in range(out.shape[0]):
        out[d] = done
    for copy in pack_copies:
        copy.wait()


def stick_read(
    queries, keys, values, lengths, offsets, routes, shares, gate, up, down, copies, experts
):
    seqs = queries.shape[0]
    wide, hidden = gate.shape[1], gate.shape[2]
    anywhere = pl.BlockSpec(memory_space=pltpu.HBM)
    vector = pl.BlockSpec(memory_space=pltpu.VMEM)
    return pl.pallas_call(
        stick_kernel,
        out_shape=(
            jax.ShapeDtypeStruct((copies, PADDED, H * HD), jnp.bfloat16),
            jax.ShapeDtypeStruct((3 * wide, hidden), jnp.bfloat16),
            jax.ShapeDtypeStruct((experts, LANES), jnp.bfloat16),
            jax.ShapeDtypeStruct((GROUP, experts), jnp.bfloat16),
            jax.ShapeDtypeStruct((GROUP, experts), jnp.bfloat16),
        ),
        in_specs=[anywhere] * 10,
        out_specs=(vector,) * 5,
        scratch_shapes=[
            pltpu.SMEM(lengths.shape, jnp.int32),
            pltpu.SMEM(offsets.shape, jnp.float32),
            pltpu.VMEM(queries.shape, jnp.bfloat16),
            pltpu.VMEM(routes.shape, jnp.int32),
            pltpu.VMEM(shares.shape, jnp.float32),
            pltpu.VMEM((8, LANES), jnp.int32),
            pltpu.VMEM((8, LANES), jnp.float32),
            pltpu.VMEM(keys.shape, jnp.bfloat16),
            pltpu.VMEM(values.shape, jnp.bfloat16),
            pltpu.VMEM((PADDED, H * HD), jnp.float32),
            pltpu.SemaphoreType.DMA((5,)),
            pltpu.SemaphoreType.DMA((seqs,)),
            pltpu.SemaphoreType.DMA((seqs,)),
            pltpu.SemaphoreType.DMA((2 + wide // LANES,)),
        ],
        compiler_params=GRANT,
        name="stick",
    )(*(
        pltpu.with_memory_space_constraint(x, pltpu.HBM)
        for x in (lengths, offsets, queries, routes, shares, keys, values, gate, up, down)
    ))


def project_kernel(reads, weight, residual, gain, bias, out):
    sources, seqs = out.shape[0], residual.shape[0] // out.shape[0]
    rows, columns = residual.shape
    mixed = reads[...]
    pairs = H // KVH
    parts = []
    for h in range(pairs):
        part = jnp.concatenate(
            [weight[h * HD : (h + 1) * HD], weight[(pairs + h) * HD : (pairs + h + 1) * HD]], axis=0
        )
        parts.append(part)
    attended = jnp.dot(
        mixed, jnp.concatenate(parts, axis=0), preferred_element_type=jnp.float32
    )
    attended = jnp.concatenate(
        [attended[t * PADDED : t * PADDED + seqs] for t in range(sources)], axis=0
    )
    before = RESIDUAL_SCALE * residual[...].astype(jnp.float32) + attended
    rest = jnp.zeros((GROUP - rows - 2, columns), jnp.float32)
    for d in range(sources):
        out[d, 0:rows] = before
        out[d, rows : rows + 1] = gain[...]
        out[d, rows + 1 : rows + 2] = bias[...]
        out[d, rows + 2 :] = rest


def project(reads, weight, residual, gain, bias, copies):
    columns = weight.shape[1]
    vector = pl.BlockSpec(memory_space=pltpu.VMEM)
    return pl.pallas_call(
        project_kernel,
        out_shape=jax.ShapeDtypeStruct((copies, GROUP, columns), jnp.float32),
        in_specs=[vector] * 5,
        out_specs=vector,
        compiler_params=GRANT,
        name="project",
    )(reads, weight, residual, gain.reshape(1, -1), bias.reshape(1, -1))


def row_moments(blocks, entries):
    total = blocks[0]
    squares = blocks[0] * blocks[0]
    for block in blocks[1:]:
        total = total + block
        squares = squares + block * block
    centre = jnp.sum(total, axis=1, keepdims=True) / entries
    spread = jnp.sum(squares, axis=1, keepdims=True) / entries - centre * centre
    return centre, lax.rsqrt(spread + EPSILON)


def norm_kernel(rows, got, dispatch, gate, up, down, whole, parcel, shared):
    blocks = []
    for t in range(got.shape[0]):
        for j in range(got.shape[2] // LANES):
            blocks.append(got[t, :, j * LANES : (j + 1) * LANES])
    centre, scale = row_moments(blocks, len(blocks) * LANES)
    normed = [
        ((block - centre) * scale * block[rows : rows + 1] + block[rows + 1 : rows + 2])
        for block in blocks
    ]
    normed = jnp.concatenate(normed, axis=1).astype(jnp.bfloat16)
    whole[...] = normed
    picked = jnp.dot(dispatch[:, 0:GROUP], normed, preferred_element_type=jnp.float32)
    parcel[...] = picked.astype(jnp.bfloat16).reshape(parcel.shape)
    gated = jnp.dot(normed, gate[...], preferred_element_type=jnp.float32)
    upped = jnp.dot(normed, up[...], preferred_element_type=jnp.float32)
    inner = (gated / (1.0 + jnp.exp(-gated)) * upped).astype(jnp.bfloat16)
    shared[...] = jnp.dot(inner, down[...], preferred_element_type=jnp.float32)


def normalize_and_pick(got, dispatch, gate, up, down, rows):
    wide = got.shape[0] * got.shape[2]
    vector = pl.BlockSpec(memory_space=pltpu.VMEM)
    return pl.pallas_call(
        functools.partial(norm_kernel, rows),
        out_shape=(
            jax.ShapeDtypeStruct((GROUP, wide), jnp.bfloat16),
            jax.ShapeDtypeStruct((dispatch.shape[0] * wide // LANES, LANES), jnp.bfloat16),
            jax.ShapeDtypeStruct((GROUP, wide), jnp.float32),
        ),
        in_specs=[vector] * 5,
        out_specs=(vector,) * 3,
        compiler_params=GRANT,
        name="norm",
    )(got, dispatch, gate, up, down)


def expert_kernel(rows, packed, side, out):
    hidden = packed.shape[1]
    wide = packed.shape[0] // 3
    count = rows.shape[0] * LANES // wide
    features = rows[...].reshape(count, wide)

    def silu_times(weights):
        joined = jnp.concatenate([weights[0:wide], weights[wide : 2 * wide]], axis=1)
        product = jnp.dot(features, joined, preferred_element_type=jnp.float32)
        gated, upped = product[:, :hidden], product[:, hidden:]
        return (gated / (1.0 + jnp.exp(-gated)) * upped).astype(jnp.bfloat16)

    both = jnp.concatenate([silu_times(packed), silu_times(side)], axis=1)
    pieces = []
    for j in range(0, wide // LANES, 2):
        at, past = 2 * wide + j * hidden, 2 * wide + (j + 1) * hidden
        down = jnp.concatenate(
            [
                jnp.concatenate([part[at : at + hidden], part[past : past + hidden]], axis=1)
                for part in (packed, side)
            ],
            axis=0,
        )
        pieces.append(jnp.dot(both, down, preferred_element_type=jnp.float32).astype(jnp.bfloat16))
    out[...] = jnp.concatenate(pieces, axis=1).reshape(out.shape)


def run_expert(rows, packed, side):
    vector = pl.BlockSpec(memory_space=pltpu.VMEM)
    return pl.pallas_call(
        expert_kernel,
        out_shape=jax.ShapeDtypeStruct(rows.shape, jnp.bfloat16),
        in_specs=[vector] * 3,
        out_specs=vector,
        compiler_params=GRANT,
        name="expert",
    )(rows, packed, side)


def combine_kernel(high, low, returned, shared, out):
    wide = shared.shape[1]
    results = returned[...].reshape(returned.shape[0] * LANES // wide, wide)
    sums = jnp.dot(high[...], results, preferred_element_type=jnp.float32)
    sums = sums + jnp.dot(low[...], results, preferred_element_type=jnp.float32)
    sums = (sums + shared[...]).astype(jnp.bfloat16)
    for d in range(out.shape[0]):
        out[d] = sums


def combine_parts(combine, returned, shared, copies):
    vector = pl.BlockSpec(memory_space=pltpu.VMEM)
    return pl.pallas_call(
        combine_kernel,
        out_shape=jax.ShapeDtypeStruct((copies, *shared.shape), jnp.bfloat16),
        in_specs=[vector] * 4,
        out_specs=vector,
        compiler_params=GRANT,
        name="combine",
    )(*combine, returned, shared)


def finish_kernel(partials, whole, gain, bias, out, after):
    rows, columns = out.shape
    blocks = []
    for j in range(whole.shape[1] // LANES):
        at = slice(j * LANES, (j + 1) * LANES)
        block = RESIDUAL_SCALE * whole[:, at].astype(jnp.float32)
        for d in range(partials.shape[0]):
            block = block + partials[d, :, at].astype(jnp.float32)
        after[:, at] = block
        blocks.append(block)
    centre, scale = row_moments(blocks, len(blocks) * LANES)
    start = pl.multiple_of(lax.axis_index("tp") * columns, columns)
    own = after[:, pl.ds(start, columns)]
    own = (own - centre) * scale * gain[...] + bias[...]
    out[...] = own[0:rows].astype(jnp.bfloat16)


def finish(partials, whole, gain, bias, rows):
    vector = pl.BlockSpec(memory_space=pltpu.VMEM)
    return pl.pallas_call(
        finish_kernel,
        out_shape=jax.ShapeDtypeStruct((rows, gain.shape[0]), jnp.bfloat16),
        in_specs=[vector] * 4,
        out_specs=vector,
        scratch_shapes=[pltpu.VMEM(whole.shape, jnp.float32)],
        compiler_params=GRANT,
        name="finish",
    )(partials, whole, gain.reshape(1, -1), bias.reshape(1, -1))


def exchanged(blocks, axis):
    return lax.all_to_all(blocks, axis, split_axis=0, concat_axis=0, tiled=True)


def body(
    residual_in,
    queries,
    cache_keys,
    cache_values,
    lengths,
    stick_offset,
    out_weight,
    norm1_gain,
    norm1_bias,
    routes,
    route_weights,
    expert_gate,
    expert_up,
    expert_down,
    shared_gate,
    shared_up,
    shared_down,
    norm2_gain,
    norm2_bias,
):
    peers = lax.axis_size("tp")
    experts = lax.axis_size("ep")
    rows, columns = residual_in.shape
    wide = columns * peers
    blocks = wide // LANES

    mixed, packed, dispatch, high, low = stick_read(
        queries, cache_keys, cache_values, lengths, stick_offset, routes.T, route_weights.T,
        expert_gate, expert_up, expert_down, peers, experts,
    )
    reads = exchanged(mixed, "tp").reshape(peers * PADDED, H * HD)
    sent = project(reads, out_weight, residual_in, norm1_gain, norm1_bias, peers)
    got = exchanged(sent, "tp")

    swaps = []
    for e in range(experts):
        for t in range(peers):
            partner = t ^ 1 if e % 2 == 0 else ((t + 1) ^ 1) - 1
            swaps.append((e * peers + t, e * peers + partner % peers))
    side = lax.ppermute(packed, ("ep", "tp"), swaps)

    whole, parcel, shared = normalize_and_pick(
        got, dispatch, shared_gate, shared_up, shared_down, rows
    )
    arrived = exchanged(parcel.reshape(experts, blocks, LANES), "ep")
    produced = run_expert(arrived.reshape(experts * blocks, LANES), packed, side)
    returned = exchanged(produced.reshape(experts, blocks, LANES), "ep")
    partial = combine_parts(
        (high, low), returned.reshape(experts * blocks, LANES), shared, peers
    )
    partials = exchanged(partial, "tp")
    return finish(partials, whole, norm2_gain, norm2_bias, rows)


def solution(mesh):
    in_specs = (
        P("ep", "tp"),
        P(("ep", "tp"), None),
        P(("ep", "tp"), None, None),
        P(("ep", "tp"), None, None),
        P(("ep", "tp")),
        P(),
        P(None, "tp"),
        P("tp"),
        P("tp"),
        P("ep", None),
        P("ep", None),
        P("ep", None, "tp"),
        P("ep", None, "tp"),
        P("ep", "tp", None),
        P(None, "tp"),
        P(None, "tp"),
        P("tp", None),
        P("tp"),
        P("tp"),
    )
    out_specs = P("ep", "tp")

    return jax.shard_map(body, mesh=mesh, in_specs=in_specs, out_specs=out_specs, check_vma=False)
```

```python
import functools

import jax
import jax.numpy as jnp
from jax import lax
from jax.experimental import pallas as pl
from jax.experimental.pallas import tpu as pltpu
from jax.sharding import PartitionSpec as P


H = 8
HD = 64
KVH = 2
CACHE = 1024
LANES = 128
BLOCKS = CACHE // LANES
PADDED = 8
GROUP = 24
GRANT = pltpu.CompilerParams(vmem_limit_bytes=12 << 20)

RESIDUAL_SCALE = 2.0**0.25
EPSILON = 1e-05


def route_tables(routes, shares, chosen, share, dispatch, high, low):
    picks, tokens = routes.shape
    chosen[...] = jnp.full(chosen.shape, -1, jnp.int32)
    share[...] = jnp.zeros(share.shape, jnp.float32)
    chosen[0:picks, 0:tokens] = routes[...]
    share[0:picks, 0:tokens] = shares[...]
    shape = (dispatch.shape[0], LANES)
    expert = lax.broadcasted_iota(jnp.int32, shape, 0)
    hits = [chosen[k : k + 1, :] == expert for k in range(picks)]
    named = jnp.zeros(shape, jnp.float32)
    for hit in hits:
        named = jnp.where(hit, 1.0, named)
    before = lax.broadcasted_iota(jnp.int32, (LANES, LANES), 0)
    token = lax.broadcasted_iota(jnp.int32, (LANES, LANES), 1)
    sooner = jnp.where(before < token, 1.0, 0.0).astype(jnp.bfloat16)
    slot = jnp.dot(named.astype(jnp.bfloat16), sooner, preferred_element_type=jnp.float32)
    mine = (lax.axis_index("tp") % 2).astype(jnp.float32)
    held = slot == mine
    dispatch[...] = jnp.where(held, named, 0.0).astype(jnp.bfloat16)
    weight = jnp.zeros(shape, jnp.float32)
    for k, hit in enumerate(hits):
        weight = jnp.where(hit & held, share[k : k + 1, :], weight)
    weight = weight.T[0 : high.shape[0]]
    upper = weight.astype(jnp.bfloat16)
    high[...] = upper
    low[...] = (weight - upper.astype(jnp.float32)).astype(jnp.bfloat16)


def stick_kernel(
    lengths_at, offsets_at, queries_at, routes_at, shares_at, keys, values, gate, up, down,
    out, packed, dispatch, high, low,
    lengths, offsets, queries, routes, shares, chosen, share, keys_vm, values_vm, reads,
    small_sems, key_sems, value_sems, pack_sems,
):
    seqs = keys.shape[0]
    wide, hidden = gate.shape[1], gate.shape[2]
    key_copies = [
        pltpu.make_async_copy(keys.at[s], keys_vm.at[s], key_sems.at[s]) for s in range(seqs)
    ]
    value_copies = [
        pltpu.make_async_copy(values.at[s], values_vm.at[s], value_sems.at[s])
        for s in range(seqs)
    ]
    pieces = [(gate.at[0], 0, wide), (up.at[0], wide, wide)]
    for j in range(wide // LANES):
        piece = down.at[0, :, pl.ds(j * LANES, LANES)]
        pieces.append((piece, 2 * wide + j * hidden, hidden))
    pack_copies = [
        pltpu.make_async_copy(piece, packed.at[pl.ds(at, rows)], pack_sems.at[i])
        for i, (piece, at, rows) in enumerate(pieces)
    ]
    small_copies = [
        pltpu.make_async_copy(source, target, small_sems.at[i])
        for i, (source, target) in enumerate(
            (
                (routes_at, routes),
                (shares_at, shares),
                (queries_at, queries),
                (lengths_at, lengths),
                (offsets_at, offsets),
            )
        )
    ]
    for copy in small_copies + key_copies + value_copies:
        copy.start()
    for copy in small_copies:
        copy.wait()
    route_tables(routes, shares, chosen, share, dispatch, high, low)

    row = lax.broadcasted_iota(jnp.int32, (H, LANES), 0)
    lane = lax.broadcasted_iota(jnp.int32, (H, LANES), 1)
    low = lane < HD
    first = row < H // KVH
    offset = jnp.zeros((H, LANES), jnp.float32)
    for h in range(H):
        offset = jnp.where(row == h, offsets[h], offset)
    wide_q = queries[...].astype(jnp.float32)
    place = lax.broadcasted_iota(jnp.int32, (LANES, 2 * LANES), 0)
    column = lax.broadcasted_iota(jnp.int32, (LANES, 2 * LANES), 1)
    later = jnp.where((place > column) | (column >= LANES), 1.0, 0.0).astype(jnp.bfloat16)

    built = []
    for s in range(seqs):
        query = jnp.zeros((H, LANES), jnp.float32)
        for h in range(H):
            pair = lax.slice(wide_q, (s, h // 2 * LANES), (s + 1, (h // 2 + 1) * LANES))
            both = jnp.broadcast_to(pair, (H, LANES))
            if h % 2 != h // (H // KVH):
                both = pltpu.roll(both, HD, 1)
            query = jnp.where(row == h, both, query)
        query = jnp.where(first == low, query, 0.0).astype(jnp.bfloat16)
        built.append(query)
    stays, takes = [], []
    for s in range(seqs):
        if s % 2 == 0:
            pair = range(s, min(s + 2, seqs))
            for p in pair:
                key_copies[p].wait()
            joined = jnp.concatenate([built[p] for p in pair], axis=0)
            keyed = jnp.concatenate([keys_vm[p] for p in pair], axis=0)
            product = lax.dot_general(
                joined, keyed, (((1,), (1,)), ((), ())), preferred_element_type=jnp.float32
            )
        i = s % 2
        scores = product[i * H : (i + 1) * H, i * CACHE : (i + 1) * CACHE]
        stay, take = [], []
        for b in range(BLOCKS):
            score = scores[:, b * LANES : (b + 1) * LANES] * HD ** (-0.5) - offset
            live = lane + b * LANES < lengths[s]
            tail = jnp.log1p(jnp.exp(-jnp.abs(score)))
            stay.append(jnp.where(live, jnp.minimum(-score, 0.0) - tail, 0.0))
            take.append(jnp.where(live, jnp.minimum(score, 0.0) - tail, -jnp.inf))
        stays.append(stay)
        takes.append(take)

    for copy in pack_copies:
        copy.start()
    rest = jnp.concatenate([stays[s][b] for b in range(BLOCKS) for s in range(seqs)], axis=0)
    sums = jnp.zeros((BLOCKS * seqs * H, 2 * LANES), jnp.float32)
    for _ in range(3):
        part = rest.astype(jnp.bfloat16)
        sums = sums + jnp.dot(part, later, preferred_element_type=jnp.float32)
        rest = rest - part.astype(jnp.float32)

    weights = [[None] * BLOCKS for _ in range(seqs)]
    for s in range(seqs):
        beyond = jnp.zeros((H, LANES), jnp.float32)
        for b in reversed(range(BLOCKS)):
            at = (b * seqs + s) * H
            after = sums[at : at + H, :LANES] + beyond
            weights[s][b] = jnp.exp(takes[s][b] + after)
            beyond = beyond + sums[at : at + H, LANES:]

    for first_seq in range(0, seqs, 2):
        pair = range(first_seq, min(first_seq + 2, seqs))
        stick = jnp.concatenate(
            [jnp.concatenate(weights[s], axis=1) for s in pair], axis=0
        ).astype(jnp.bfloat16)
        for s in pair:
            value_copies[s].wait()
        both = jnp.concatenate([values_vm[s] for s in pair], axis=1)
        product = jnp.dot(stick, both, preferred_element_type=jnp.float32)
        for i, s in enumerate(pair):
            mixed = product[i * H : (i + 1) * H, i * LANES : (i + 1) * LANES]
            mixed = jnp.where(low, mixed, pltpu.roll(mixed, H // KVH, 0))
            for h in range(H // KVH):
                reads[s : s + 1, h * LANES : (h + 1) * LANES] = mixed[h : h + 1, :]
    reads[seqs:, :] = jnp.zeros((reads.shape[0] - seqs, H * HD), jnp.float32)
    done = reads[...].astype(jnp.bfloat16)
    for d in range(out.shape[0]):
        out[d] = done
    for copy in pack_copies:
        copy.wait()


def stick_read(
    queries, keys, values, lengths, offsets, routes, shares, gate, up, down, copies, experts
):
    seqs = queries.shape[0]
    wide, hidden = gate.shape[1], gate.shape[2]
    anywhere = pl.BlockSpec(memory_space=pltpu.HBM)
    vector = pl.BlockSpec(memory_space=pltpu.VMEM)
    return pl.pallas_call(
        stick_kernel,
        out_shape=(
            jax.ShapeDtypeStruct((copies, PADDED, H * HD), jnp.bfloat16),
            jax.ShapeDtypeStruct((3 * wide, hidden), jnp.bfloat16),
            jax.ShapeDtypeStruct((experts, LANES), jnp.bfloat16),
            jax.ShapeDtypeStruct((GROUP, experts), jnp.bfloat16),
            jax.ShapeDtypeStruct((GROUP, experts), jnp.bfloat16),
        ),
        in_specs=[anywhere] * 10,
        out_specs=(vector,) * 5,
        scratch_shapes=[
            pltpu.SMEM(lengths.shape, jnp.int32),
            pltpu.SMEM(offsets.shape, jnp.float32),
            pltpu.VMEM(queries.shape, jnp.bfloat16),
            pltpu.VMEM(routes.shape, jnp.int32),
            pltpu.VMEM(shares.shape, jnp.float32),
            pltpu.VMEM((8, LANES), jnp.int32),
            pltpu.VMEM((8, LANES), jnp.float32),
            pltpu.VMEM(keys.shape, jnp.bfloat16),
            pltpu.VMEM(values.shape, jnp.bfloat16),
            pltpu.VMEM((PADDED, H * HD), jnp.float32),
            pltpu.SemaphoreType.DMA((5,)),
            pltpu.SemaphoreType.DMA((seqs,)),
            pltpu.SemaphoreType.DMA((seqs,)),
            pltpu.SemaphoreType.DMA((2 + wide // LANES,)),
        ],
        compiler_params=GRANT,
        name="stick",
    )(*(
        pltpu.with_memory_space_constraint(x, pltpu.HBM)
        for x in (lengths, offsets, queries, routes, shares, keys, values, gate, up, down)
    ))


def project_kernel(reads, weight, residual, gain, bias, out):
    sources, seqs = out.shape[0], residual.shape[0] // out.shape[0]
    rows, columns = residual.shape
    mixed = reads[...]
    pairs = H // KVH
    parts = []
    for h in range(pairs):
        part = jnp.concatenate(
            [weight[h * HD : (h + 1) * HD], weight[(pairs + h) * HD : (pairs + h + 1) * HD]], axis=0
        )
        parts.append(part)
    attended = jnp.dot(
        mixed, jnp.concatenate(parts, axis=0), preferred_element_type=jnp.float32
    )
    attended = jnp.concatenate(
        [attended[t * PADDED : t * PADDED + seqs] for t in range(sources)], axis=0
    )
    before = RESIDUAL_SCALE * residual[...].astype(jnp.float32) + attended
    rest = jnp.zeros((GROUP - rows - 2, columns), jnp.float32)
    for d in range(sources):
        out[d, 0:rows] = before
        out[d, rows : rows + 1] = gain[...]
        out[d, rows + 1 : rows + 2] = bias[...]
        out[d, rows + 2 :] = rest


def project(reads, weight, residual, gain, bias, copies):
    columns = weight.shape[1]
    vector = pl.BlockSpec(memory_space=pltpu.VMEM)
    return pl.pallas_call(
        project_kernel,
        out_shape=jax.ShapeDtypeStruct((copies, GROUP, columns), jnp.float32),
        in_specs=[vector] * 5,
        out_specs=vector,
        compiler_params=GRANT,
        name="project",
    )(reads, weight, residual, gain.reshape(1, -1), bias.reshape(1, -1))


def row_moments(blocks, entries):
    total = blocks[0]
    squares = blocks[0] * blocks[0]
    for block in blocks[1:]:
        total = total + block
        squares = squares + block * block
    centre = jnp.sum(total, axis=1, keepdims=True) / entries
    spread = jnp.sum(squares, axis=1, keepdims=True) / entries - centre * centre
    return centre, lax.rsqrt(spread + EPSILON)


def norm_kernel(rows, got, dispatch, gate, up, down, whole, parcel, shared):
    blocks = []
    for t in range(got.shape[0]):
        for j in range(got.shape[2] // LANES):
            blocks.append(got[t, :, j * LANES : (j + 1) * LANES])
    centre, scale = row_moments(blocks, len(blocks) * LANES)
    normed = [
        ((block - centre) * scale * block[rows : rows + 1] + block[rows + 1 : rows + 2])
        for block in blocks
    ]
    token = lax.broadcasted_iota(jnp.int32, normed[0].shape, 0) < rows
    normed = [jnp.where(token, block, 0.0) for block in normed]
    normed = jnp.concatenate(normed, axis=1).astype(jnp.bfloat16)
    wide = normed.shape[1]
    whole[...] = normed.reshape(GROUP * wide // LANES, LANES)[0 : whole.shape[0]]
    picked = jnp.dot(dispatch[:, 0:GROUP], normed, preferred_element_type=jnp.float32)
    parcel[...] = picked.astype(jnp.bfloat16).reshape(parcel.shape)
    gated = jnp.dot(normed, gate[...], preferred_element_type=jnp.float32)
    upped = jnp.dot(normed, up[...], preferred_element_type=jnp.float32)
    inner = (gated / (1.0 + jnp.exp(-gated)) * upped).astype(jnp.bfloat16)
    shared[...] = jnp.dot(inner, down[...], preferred_element_type=jnp.float32)


def normalize_and_pick(got, dispatch, gate, up, down, rows):
    wide = got.shape[0] * got.shape[2]
    vector = pl.BlockSpec(memory_space=pltpu.VMEM)
    return pl.pallas_call(
        functools.partial(norm_kernel, rows),
        out_shape=(
            jax.ShapeDtypeStruct((rows * wide // LANES, LANES), jnp.bfloat16),
            jax.ShapeDtypeStruct((dispatch.shape[0] * wide // LANES, LANES), jnp.bfloat16),
            jax.ShapeDtypeStruct((GROUP, wide), jnp.float32),
        ),
        in_specs=[vector] * 5,
        out_specs=(vector,) * 3,
        compiler_params=GRANT,
        name="norm",
    )(got, dispatch, gate, up, down)


def expert_kernel(rows, packed, side, out):
    hidden = packed.shape[1]
    wide = packed.shape[0] // 3
    count = rows.shape[0] * LANES // wide
    features = rows[...].reshape(count, wide)

    def silu_times(weights):
        joined = jnp.concatenate([weights[0:wide], weights[wide : 2 * wide]], axis=1)
        product = jnp.dot(features, joined, preferred_element_type=jnp.float32)
        gated, upped = product[:, :hidden], product[:, hidden:]
        return (gated / (1.0 + jnp.exp(-gated)) * upped).astype(jnp.bfloat16)

    both = jnp.concatenate([silu_times(packed), silu_times(side)], axis=1)
    pieces = []
    for j in range(0, wide // LANES, 2):
        at, past = 2 * wide + j * hidden, 2 * wide + (j + 1) * hidden
        down = jnp.concatenate(
            [
                jnp.concatenate([part[at : at + hidden], part[past : past + hidden]], axis=1)
                for part in (packed, side)
            ],
            axis=0,
        )
        pieces.append(jnp.dot(both, down, preferred_element_type=jnp.float32).astype(jnp.bfloat16))
    out[...] = jnp.concatenate(pieces, axis=1).reshape(out.shape)


def run_expert(rows, packed, side):
    vector = pl.BlockSpec(memory_space=pltpu.VMEM)
    return pl.pallas_call(
        expert_kernel,
        out_shape=jax.ShapeDtypeStruct(rows.shape, jnp.bfloat16),
        in_specs=[vector] * 3,
        out_specs=vector,
        compiler_params=GRANT,
        name="expert",
    )(rows, packed, side)


def combine_kernel(high, low, returned, shared, out):
    wide = shared.shape[1]
    results = returned[...].reshape(returned.shape[0] * LANES // wide, wide)
    sums = jnp.dot(high[...], results, preferred_element_type=jnp.float32)
    sums = sums + jnp.dot(low[...], results, preferred_element_type=jnp.float32)
    sums = (sums + shared[...]).astype(jnp.bfloat16)
    sums = sums.reshape(sums.shape[0] * wide // LANES, LANES)[0 : out.shape[1]]
    for d in range(out.shape[0]):
        out[d] = sums


def combine_parts(combine, returned, shared, copies, rows):
    vector = pl.BlockSpec(memory_space=pltpu.VMEM)
    return pl.pallas_call(
        combine_kernel,
        out_shape=jax.ShapeDtypeStruct(
            (copies, rows * shared.shape[1] // LANES, LANES), jnp.bfloat16
        ),
        in_specs=[vector] * 4,
        out_specs=vector,
        compiler_params=GRANT,
        name="combine",
    )(*combine, returned, shared)


def finish_kernel(partials, whole, gain, bias, out, after):
    _, columns = out.shape
    blocks = after.shape[1]
    value = RESIDUAL_SCALE * whole[...].astype(jnp.float32)
    for d in range(partials.shape[0]):
        value = value + partials[d].astype(jnp.float32)
    value = value.reshape(after.shape)
    entries = blocks * LANES
    centre = jnp.sum(value, axis=(1, 2), keepdims=True) / entries
    spread = jnp.sum(value * value, axis=(1, 2), keepdims=True) / entries - centre * centre
    after[...] = (value - centre) * lax.rsqrt(spread + EPSILON)
    pieces = columns // LANES
    for j in range(pieces):
        at = slice(j * LANES, (j + 1) * LANES)
        own = after[:, lax.axis_index("tp") * pieces + j, :]
        out[:, at] = (own * gain[:, at] + bias[:, at]).astype(jnp.bfloat16)


def finish(partials, whole, gain, bias, rows):
    vector = pl.BlockSpec(memory_space=pltpu.VMEM)
    return pl.pallas_call(
        finish_kernel,
        out_shape=jax.ShapeDtypeStruct((rows, gain.shape[0]), jnp.bfloat16),
        in_specs=[vector] * 4,
        out_specs=vector,
        scratch_shapes=[pltpu.VMEM((rows, whole.shape[0] // rows, LANES), jnp.float32)],
        compiler_params=GRANT,
        name="finish",
    )(partials, whole, gain.reshape(1, -1), bias.reshape(1, -1))


def fetch_kernel(after, *refs):
    count = (len(refs) - 1) // 2
    sources, targets, sems = refs[:count], refs[count:-1], refs[-1]
    copies = [
        pltpu.make_async_copy(source, target, sems.at[i])
        for i, (source, target) in enumerate(zip(sources, targets))
    ]
    for copy in copies:
        copy.start()
    for copy in copies:
        copy.wait()


def fetched(after, *arrays):
    anywhere = pl.BlockSpec(memory_space=pltpu.HBM)
    vector = pl.BlockSpec(memory_space=pltpu.VMEM)
    return pl.pallas_call(
        fetch_kernel,
        out_shape=tuple(jax.ShapeDtypeStruct(a.shape, a.dtype) for a in arrays),
        in_specs=[anywhere] * (1 + len(arrays)),
        out_specs=(vector,) * len(arrays),
        scratch_shapes=[pltpu.SemaphoreType.DMA((len(arrays),))],
        compiler_params=GRANT,
        name="fetch",
    )(*(pltpu.with_memory_space_constraint(a, pltpu.HBM) for a in (after, *arrays)))


def exchanged(blocks, axis):
    return lax.all_to_all(blocks, axis, split_axis=0, concat_axis=0, tiled=True)


def body(
    residual_in,
    queries,
    cache_keys,
    cache_values,
    lengths,
    stick_offset,
    out_weight,
    norm1_gain,
    norm1_bias,
    routes,
    route_weights,
    expert_gate,
    expert_up,
    expert_down,
    shared_gate,
    shared_up,
    shared_down,
    norm2_gain,
    norm2_bias,
):
    peers = lax.axis_size("tp")
    experts = lax.axis_size("ep")
    rows, columns = residual_in.shape
    wide = columns * peers
    blocks = wide // LANES

    mixed, packed, dispatch, high, low = stick_read(
        queries, cache_keys, cache_values, lengths, stick_offset, routes.T, route_weights.T,
        expert_gate, expert_up, expert_down, peers, experts,
    )
    reads = exchanged(mixed, "tp").reshape(peers * PADDED, H * HD)
    sent = project(reads, out_weight, residual_in, norm1_gain, norm1_bias, peers)
    got = exchanged(sent, "tp")

    swaps = []
    for e in range(experts):
        for t in range(peers):
            partner = t ^ 1 if e % 2 == 0 else ((t + 1) ^ 1) - 1
            swaps.append((e * peers + t, e * peers + partner % peers))
    side = lax.ppermute(packed, ("ep", "tp"), swaps)

    shared_parts = fetched(sent, shared_gate, shared_up, shared_down)
    whole, parcel, shared = normalize_and_pick(got, dispatch, *shared_parts, rows)
    arrived = exchanged(parcel.reshape(experts, blocks, LANES), "ep")
    produced = run_expert(arrived.reshape(experts * blocks, LANES), packed, side)
    returned = exchanged(produced.reshape(experts, blocks, LANES), "ep")
    partial = combine_parts(
        (high, low), returned.reshape(experts * blocks, LANES), shared, peers, rows
    )
    partials = exchanged(partial, "tp")
    return finish(partials, whole, norm2_gain, norm2_bias, rows)


def solution(mesh):
    in_specs = (
        P("ep", "tp"),
        P(("ep", "tp"), None),
        P(("ep", "tp"), None, None),
        P(("ep", "tp"), None, None),
        P(("ep", "tp")),
        P(),
        P(None, "tp"),
        P("tp"),
        P("tp"),
        P("ep", None),
        P("ep", None),
        P("ep", None, "tp"),
        P("ep", None, "tp"),
        P("ep", "tp", None),
        P(None, "tp"),
        P(None, "tp"),
        P("tp", None),
        P("tp"),
        P("tp"),
    )
    out_specs = P("ep", "tp")

    return jax.shard_map(body, mesh=mesh, in_specs=in_specs, out_specs=out_specs, check_vma=False)
```

```python
import functools

import jax
import jax.numpy as jnp
from jax import lax
from jax.experimental import pallas as pl
from jax.experimental.pallas import tpu as pltpu
from jax.sharding import PartitionSpec as P


H = 8
HD = 64
KVH = 2
CACHE = 1024
LANES = 128
BLOCKS = CACHE // LANES
PADDED = 8
GROUP = 24
GRANT = pltpu.CompilerParams(vmem_limit_bytes=12 << 20)

RESIDUAL_SCALE = 2.0**0.25
EPSILON = 1e-05


def route_tables(routes, shares, chosen, share, dispatch, high, low):
    picks, tokens = routes.shape
    chosen[...] = jnp.full(chosen.shape, -1, jnp.int32)
    share[...] = jnp.zeros(share.shape, jnp.float32)
    chosen[0:picks, 0:tokens] = routes[...]
    share[0:picks, 0:tokens] = shares[...]
    shape = (dispatch.shape[0], LANES)
    expert = lax.broadcasted_iota(jnp.int32, shape, 0)
    hits = [chosen[k : k + 1, :] == expert for k in range(picks)]
    named = jnp.zeros(shape, jnp.float32)
    for hit in hits:
        named = jnp.where(hit, 1.0, named)
    before = lax.broadcasted_iota(jnp.int32, (LANES, LANES), 0)
    token = lax.broadcasted_iota(jnp.int32, (LANES, LANES), 1)
    sooner = jnp.where(before < token, 1.0, 0.0).astype(jnp.bfloat16)
    slot = jnp.dot(named.astype(jnp.bfloat16), sooner, preferred_element_type=jnp.float32)
    mine = (lax.axis_index("tp") % 2).astype(jnp.float32)
    held = slot == mine
    dispatch[...] = jnp.where(held, named, 0.0).astype(jnp.bfloat16)
    weight = jnp.zeros(shape, jnp.float32)
    for k, hit in enumerate(hits):
        weight = jnp.where(hit & held, share[k : k + 1, :], weight)
    weight = weight.T[0 : high.shape[0]]
    upper = weight.astype(jnp.bfloat16)
    high[...] = upper
    low[...] = (weight - upper.astype(jnp.float32)).astype(jnp.bfloat16)


def stick_kernel(
    lengths_at, offsets_at, queries_at, routes_at, shares_at, keys, values, gate, up, down,
    out, packed, dispatch, high, low,
    lengths, offsets, queries, routes, shares, chosen, share, keys_vm, values_vm, reads,
    small_sems, key_sems, value_sems, pack_sems,
):
    seqs = keys.shape[0]
    wide, hidden = gate.shape[1], gate.shape[2]
    key_copies = [
        pltpu.make_async_copy(keys.at[s], keys_vm.at[s], key_sems.at[s]) for s in range(seqs)
    ]
    value_copies = [
        pltpu.make_async_copy(values.at[s], values_vm.at[s], value_sems.at[s])
        for s in range(seqs)
    ]
    pieces = [(gate.at[0], 0, wide), (up.at[0], wide, wide)]
    for j in range(wide // LANES):
        piece = down.at[0, :, pl.ds(j * LANES, LANES)]
        pieces.append((piece, 2 * wide + j * hidden, hidden))
    pack_copies = [
        pltpu.make_async_copy(piece, packed.at[pl.ds(at, rows)], pack_sems.at[i])
        for i, (piece, at, rows) in enumerate(pieces)
    ]
    small_copies = [
        pltpu.make_async_copy(source, target, small_sems.at[i])
        for i, (source, target) in enumerate(
            (
                (routes_at, routes),
                (shares_at, shares),
                (queries_at, queries),
                (lengths_at, lengths),
                (offsets_at, offsets),
            )
        )
    ]
    for copy in small_copies + key_copies + value_copies:
        copy.start()
    for copy in small_copies:
        copy.wait()
    route_tables(routes, shares, chosen, share, dispatch, high, low)

    row = lax.broadcasted_iota(jnp.int32, (H, LANES), 0)
    lane = lax.broadcasted_iota(jnp.int32, (H, LANES), 1)
    low = lane < HD
    first = row < H // KVH
    offset = jnp.zeros((H, LANES), jnp.float32)
    for h in range(H):
        offset = jnp.where(row == h, offsets[h], offset)
    wide_q = queries[...].astype(jnp.float32)
    place = lax.broadcasted_iota(jnp.int32, (LANES, 2 * LANES), 0)
    column = lax.broadcasted_iota(jnp.int32, (LANES, 2 * LANES), 1)
    later = jnp.where((place > column) | (column >= LANES), 1.0, 0.0).astype(jnp.bfloat16)

    built = []
    for s in range(seqs):
        query = jnp.zeros((H, LANES), jnp.float32)
        for h in range(H):
            pair = lax.slice(wide_q, (s, h // 2 * LANES), (s + 1, (h // 2 + 1) * LANES))
            both = jnp.broadcast_to(pair, (H, LANES))
            if h % 2 != h // (H // KVH):
                both = pltpu.roll(both, HD, 1)
            query = jnp.where(row == h, both, query)
        query = jnp.where(first == low, query, 0.0).astype(jnp.bfloat16)
        built.append(query)
    stays, takes = [], []
    for s in range(seqs):
        if s % 2 == 0:
            pair = range(s, min(s + 2, seqs))
            for p in pair:
                key_copies[p].wait()
            joined = jnp.concatenate([built[p] for p in pair], axis=0)
            keyed = jnp.concatenate([keys_vm[p] for p in pair], axis=0)
            product = lax.dot_general(
                joined, keyed, (((1,), (1,)), ((), ())), preferred_element_type=jnp.float32
            )
        i = s % 2
        scores = product[i * H : (i + 1) * H, i * CACHE : (i + 1) * CACHE]
        stay, take = [], []
        for b in range(BLOCKS):
            score = scores[:, b * LANES : (b + 1) * LANES] * HD ** (-0.5) - offset
            live = lane + b * LANES < lengths[s]
            tail = jnp.log1p(jnp.exp(-jnp.abs(score)))
            stay.append(jnp.where(live, jnp.minimum(-score, 0.0) - tail, 0.0))
            take.append(jnp.where(live, jnp.minimum(score, 0.0) - tail, -jnp.inf))
        stays.append(stay)
        takes.append(take)

    for copy in pack_copies:
        copy.start()
    rest = jnp.concatenate([stays[s][b] for b in range(BLOCKS) for s in range(seqs)], axis=0)
    sums = jnp.zeros((BLOCKS * seqs * H, 2 * LANES), jnp.float32)
    for _ in range(3):
        part = rest.astype(jnp.bfloat16)
        sums = sums + jnp.dot(part, later, preferred_element_type=jnp.float32)
        rest = rest - part.astype(jnp.float32)

    weights = [[None] * BLOCKS for _ in range(seqs)]
    for s in range(seqs):
        beyond = jnp.zeros((H, LANES), jnp.float32)
        for b in reversed(range(BLOCKS)):
            at = (b * seqs + s) * H
            after = sums[at : at + H, :LANES] + beyond
            weights[s][b] = jnp.exp(takes[s][b] + after)
            beyond = beyond + sums[at : at + H, LANES:]

    for first_seq in range(0, seqs, 2):
        pair = range(first_seq, min(first_seq + 2, seqs))
        stick = jnp.concatenate(
            [jnp.concatenate(weights[s], axis=1) for s in pair], axis=0
        ).astype(jnp.bfloat16)
        for s in pair:
            value_copies[s].wait()
        both = jnp.concatenate([values_vm[s] for s in pair], axis=1)
        product = jnp.dot(stick, both, preferred_element_type=jnp.float32)
        for i, s in enumerate(pair):
            mixed = product[i * H : (i + 1) * H, i * LANES : (i + 1) * LANES]
            mixed = jnp.where(low, mixed, pltpu.roll(mixed, H // KVH, 0))
            for h in range(H // KVH):
                reads[s : s + 1, h * LANES : (h + 1) * LANES] = mixed[h : h + 1, :]
    reads[seqs:, :] = jnp.zeros((reads.shape[0] - seqs, H * HD), jnp.float32)
    done = reads[...].astype(jnp.bfloat16)
    for d in range(out.shape[0]):
        out[d] = done
    for copy in pack_copies:
        copy.wait()


def stick_read(
    queries, keys, values, lengths, offsets, routes, shares, gate, up, down, copies, experts
):
    seqs = queries.shape[0]
    wide, hidden = gate.shape[1], gate.shape[2]
    anywhere = pl.BlockSpec(memory_space=pltpu.HBM)
    vector = pl.BlockSpec(memory_space=pltpu.VMEM)
    return pl.pallas_call(
        stick_kernel,
        out_shape=(
            jax.ShapeDtypeStruct((copies, PADDED, H * HD), jnp.bfloat16),
            jax.ShapeDtypeStruct((3 * wide, hidden), jnp.bfloat16),
            jax.ShapeDtypeStruct((experts, LANES), jnp.bfloat16),
            jax.ShapeDtypeStruct((GROUP, experts), jnp.bfloat16),
            jax.ShapeDtypeStruct((GROUP, experts), jnp.bfloat16),
        ),
        in_specs=[anywhere] * 10,
        out_specs=(vector,) * 5,
        scratch_shapes=[
            pltpu.SMEM(lengths.shape, jnp.int32),
            pltpu.SMEM(offsets.shape, jnp.float32),
            pltpu.VMEM(queries.shape, jnp.bfloat16),
            pltpu.VMEM(routes.shape, jnp.int32),
            pltpu.VMEM(shares.shape, jnp.float32),
            pltpu.VMEM((8, LANES), jnp.int32),
            pltpu.VMEM((8, LANES), jnp.float32),
            pltpu.VMEM(keys.shape, jnp.bfloat16),
            pltpu.VMEM(values.shape, jnp.bfloat16),
            pltpu.VMEM((PADDED, H * HD), jnp.float32),
            pltpu.SemaphoreType.DMA((5,)),
            pltpu.SemaphoreType.DMA((seqs,)),
            pltpu.SemaphoreType.DMA((seqs,)),
            pltpu.SemaphoreType.DMA((2 + wide // LANES,)),
        ],
        compiler_params=GRANT,
        name="stick",
    )(*(
        pltpu.with_memory_space_constraint(x, pltpu.HBM)
        for x in (lengths, offsets, queries, routes, shares, keys, values, gate, up, down)
    ))


def project_kernel(reads, weight, residual, gain, bias, out):
    sources, seqs = out.shape[0], residual.shape[0] // out.shape[0]
    rows, columns = residual.shape
    mixed = reads[...]
    pairs = H // KVH
    parts = []
    for h in range(pairs):
        part = jnp.concatenate(
            [weight[h * HD : (h + 1) * HD], weight[(pairs + h) * HD : (pairs + h + 1) * HD]], axis=0
        )
        parts.append(part)
    attended = jnp.dot(
        mixed, jnp.concatenate(parts, axis=0), preferred_element_type=jnp.float32
    )
    attended = jnp.concatenate(
        [attended[t * PADDED : t * PADDED + seqs] for t in range(sources)], axis=0
    )
    before = RESIDUAL_SCALE * residual[...].astype(jnp.float32) + attended
    rest = jnp.zeros((GROUP - rows - 2, columns), jnp.float32)
    for d in range(sources):
        out[d, 0:rows] = before
        out[d, rows : rows + 1] = gain[...]
        out[d, rows + 1 : rows + 2] = bias[...]
        out[d, rows + 2 :] = rest


def project(reads, weight, residual, gain, bias, copies):
    columns = weight.shape[1]
    vector = pl.BlockSpec(memory_space=pltpu.VMEM)
    return pl.pallas_call(
        project_kernel,
        out_shape=jax.ShapeDtypeStruct((copies, GROUP, columns), jnp.float32),
        in_specs=[vector] * 5,
        out_specs=vector,
        compiler_params=GRANT,
        name="project",
    )(reads, weight, residual, gain.reshape(1, -1), bias.reshape(1, -1))


def row_moments(blocks, entries):
    total = blocks[0]
    squares = blocks[0] * blocks[0]
    for block in blocks[1:]:
        total = total + block
        squares = squares + block * block
    centre = jnp.sum(total, axis=1, keepdims=True) / entries
    spread = jnp.sum(squares, axis=1, keepdims=True) / entries - centre * centre
    return centre, lax.rsqrt(spread + EPSILON)


def norm_kernel(rows, got, dispatch, gate, up, down, whole, parcel, shared):
    blocks = []
    for t in range(got.shape[0]):
        for j in range(got.shape[2] // LANES):
            blocks.append(got[t, :, j * LANES : (j + 1) * LANES])
    centre, scale = row_moments(blocks, len(blocks) * LANES)
    normed = [
        ((block - centre) * scale * block[rows : rows + 1] + block[rows + 1 : rows + 2])
        for block in blocks
    ]
    token = lax.broadcasted_iota(jnp.int32, normed[0].shape, 0) < rows
    normed = [jnp.where(token, block, 0.0) for block in normed]
    normed = jnp.concatenate(normed, axis=1).astype(jnp.bfloat16)
    wide = normed.shape[1]
    whole[...] = normed.reshape(GROUP * wide // LANES, LANES)[0 : whole.shape[0]]
    picked = jnp.dot(dispatch[:, 0:GROUP], normed, preferred_element_type=jnp.float32)
    parcel[...] = picked.astype(jnp.bfloat16).reshape(parcel.shape)
    gated = jnp.dot(normed, gate[...], preferred_element_type=jnp.float32)
    upped = jnp.dot(normed, up[...], preferred_element_type=jnp.float32)
    inner = (gated / (1.0 + jnp.exp(-gated)) * upped).astype(jnp.bfloat16)
    shared[...] = jnp.dot(inner, down[...], preferred_element_type=jnp.float32)


def normalize_and_pick(got, dispatch, gate, up, down, rows):
    wide = got.shape[0] * got.shape[2]
    vector = pl.BlockSpec(memory_space=pltpu.VMEM)
    return pl.pallas_call(
        functools.partial(norm_kernel, rows),
        out_shape=(
            jax.ShapeDtypeStruct((rows * wide // LANES, LANES), jnp.bfloat16),
            jax.ShapeDtypeStruct((dispatch.shape[0] * wide // LANES, LANES), jnp.bfloat16),
            jax.ShapeDtypeStruct((GROUP, wide), jnp.float32),
        ),
        in_specs=[vector] * 5,
        out_specs=(vector,) * 3,
        compiler_params=GRANT,
        name="norm",
    )(got, dispatch, gate, up, down)


def expert_kernel(rows, packed, side, out):
    hidden = packed.shape[1]
    wide = packed.shape[0] // 3
    count = rows.shape[0] * LANES // wide
    features = rows[...].reshape(count, wide)

    def silu_times(weights):
        joined = jnp.concatenate([weights[0:wide], weights[wide : 2 * wide]], axis=1)
        product = jnp.dot(features, joined, preferred_element_type=jnp.float32)
        gated, upped = product[:, :hidden], product[:, hidden:]
        return (gated / (1.0 + jnp.exp(-gated)) * upped).astype(jnp.bfloat16)

    both = jnp.concatenate([silu_times(packed), silu_times(side)], axis=1)
    pieces = []
    for j in range(0, wide // LANES, 2):
        at, past = 2 * wide + j * hidden, 2 * wide + (j + 1) * hidden
        down = jnp.concatenate(
            [
                jnp.concatenate([part[at : at + hidden], part[past : past + hidden]], axis=1)
                for part in (packed, side)
            ],
            axis=0,
        )
        pieces.append(jnp.dot(both, down, preferred_element_type=jnp.float32).astype(jnp.bfloat16))
    out[...] = jnp.concatenate(pieces, axis=1).reshape(out.shape)


def run_expert(rows, packed, side):
    vector = pl.BlockSpec(memory_space=pltpu.VMEM)
    return pl.pallas_call(
        expert_kernel,
        out_shape=jax.ShapeDtypeStruct(rows.shape, jnp.bfloat16),
        in_specs=[vector] * 3,
        out_specs=vector,
        compiler_params=GRANT,
        name="expert",
    )(rows, packed, side)


def combine_kernel(high, low, returned, shared, out):
    wide = shared.shape[1]
    results = returned[...].reshape(returned.shape[0] * LANES // wide, wide)
    sums = jnp.dot(high[...], results, preferred_element_type=jnp.float32)
    sums = sums + jnp.dot(low[...], results, preferred_element_type=jnp.float32)
    sums = (sums + shared[...]).astype(jnp.bfloat16)
    sums = sums.reshape(sums.shape[0] * wide // LANES, LANES)[0 : out.shape[1]]
    for d in range(out.shape[0]):
        out[d] = sums


def combine_parts(combine, returned, shared, copies, rows):
    vector = pl.BlockSpec(memory_space=pltpu.VMEM)
    return pl.pallas_call(
        combine_kernel,
        out_shape=jax.ShapeDtypeStruct(
            (copies, rows * shared.shape[1] // LANES, LANES), jnp.bfloat16
        ),
        in_specs=[vector] * 4,
        out_specs=vector,
        compiler_params=GRANT,
        name="combine",
    )(*combine, returned, shared)


def finish_kernel(partials, whole, gain, bias, out, after):
    _, columns = out.shape
    blocks = after.shape[1]
    value = RESIDUAL_SCALE * whole[...].astype(jnp.float32)
    for d in range(partials.shape[0]):
        value = value + partials[d].astype(jnp.float32)
    value = value.reshape(after.shape)
    entries = blocks * LANES
    centre = jnp.sum(value, axis=(1, 2), keepdims=True) / entries
    spread = jnp.sum(value * value, axis=(1, 2), keepdims=True) / entries - centre * centre
    after[...] = (value - centre) * lax.rsqrt(spread + EPSILON)
    pieces = columns // LANES
    for j in range(pieces):
        at = slice(j * LANES, (j + 1) * LANES)
        own = after[:, lax.axis_index("tp") * pieces + j, :]
        out[:, at] = (own * gain[:, at] + bias[:, at]).astype(jnp.bfloat16)


def finish(partials, whole, gain, bias, rows):
    vector = pl.BlockSpec(memory_space=pltpu.VMEM)
    return pl.pallas_call(
        finish_kernel,
        out_shape=jax.ShapeDtypeStruct((rows, gain.shape[0]), jnp.bfloat16),
        in_specs=[vector] * 4,
        out_specs=vector,
        scratch_shapes=[pltpu.VMEM((rows, whole.shape[0] // rows, LANES), jnp.float32)],
        compiler_params=GRANT,
        name="finish",
    )(partials, whole, gain.reshape(1, -1), bias.reshape(1, -1))


def exchanged(blocks, axis):
    return lax.all_to_all(blocks, axis, split_axis=0, concat_axis=0, tiled=True)


def body(
    residual_in,
    queries,
    cache_keys,
    cache_values,
    lengths,
    stick_offset,
    out_weight,
    norm1_gain,
    norm1_bias,
    routes,
    route_weights,
    expert_gate,
    expert_up,
    expert_down,
    shared_gate,
    shared_up,
    shared_down,
    norm2_gain,
    norm2_bias,
):
    peers = lax.axis_size("tp")
    experts = lax.axis_size("ep")
    rows, columns = residual_in.shape
    wide = columns * peers
    blocks = wide // LANES

    mixed, packed, dispatch, high, low = stick_read(
        queries, cache_keys, cache_values, lengths, stick_offset, routes.T, route_weights.T,
        expert_gate, expert_up, expert_down, peers, experts,
    )
    reads = exchanged(mixed, "tp").reshape(peers * PADDED, H * HD)
    sent = project(reads, out_weight, residual_in, norm1_gain, norm1_bias, peers)
    got = exchanged(sent, "tp")

    swaps = []
    for e in range(experts):
        for t in range(peers):
            partner = t ^ 1 if e % 2 == 0 else ((t + 1) ^ 1) - 1
            swaps.append((e * peers + t, e * peers + partner % peers))
    side = lax.ppermute(packed, ("ep", "tp"), swaps)

    whole, parcel, shared = normalize_and_pick(
        got, dispatch, shared_gate, shared_up, shared_down, rows
    )
    arrived = exchanged(parcel.reshape(experts, blocks, LANES), "ep")
    produced = run_expert(arrived.reshape(experts * blocks, LANES), packed, side)
    returned = exchanged(produced.reshape(experts, blocks, LANES), "ep")
    partial = combine_parts(
        (high, low), returned.reshape(experts * blocks, LANES), shared, peers, rows
    )
    partials = exchanged(partial, "tp")
    return finish(partials, whole, norm2_gain, norm2_bias, rows)


def solution(mesh):
    in_specs = (
        P("ep", "tp"),
        P(("ep", "tp"), None),
        P(("ep", "tp"), None, None),
        P(("ep", "tp"), None, None),
        P(("ep", "tp")),
        P(),
        P(None, "tp"),
        P("tp"),
        P("tp"),
        P("ep", None),
        P("ep", None),
        P("ep", None, "tp"),
        P("ep", None, "tp"),
        P("ep", "tp", None),
        P(None, "tp"),
        P(None, "tp"),
        P("tp", None),
        P("tp"),
        P("tp"),
    )
    out_specs = P("ep", "tp")

    return jax.shard_map(body, mesh=mesh, in_specs=in_specs, out_specs=out_specs, check_vma=False)
```
